256 devices in a mesh: sp: 64 (over z, x, core), tp: 4 (over y).
Axes of the slice: x: 4, y: 4, z: 8, core: 2. Of those that a mesh axis runs over, the one named last changes fastest.
Arguments:
- mixer_input: bfloat16 [32768, 2048], P('sp', 'tp'), may hold values from -6 to 6
- residual: bfloat16 [32768, 2048], P(('sp', 'tp')), may hold values from -6 to 6
- log_step: float32 [128], P('tp'), may hold values from -3.9 to -2.3
- rate_real: float32 [128, 64], P('tp'), may hold values from -1.5 to 0, as said below
- rate_imag: float32 [128, 64], P('tp'), may hold values from 2 to 30
- damping: float32 [32768, 128], P('sp', 'tp'), may hold values from -2 to 0, as said below
- in_map: float32 [2, 128, 64, 16], P(None, 'tp'), may hold values from -1 to 1
- out_map: float32 [2, 128, 16, 64], P(None, 'tp'), may hold values from -0.75 to 0.75
- skip: float32 [2048], P('tp'), may hold values from -3 to 3
- w_out: bfloat16 [2048, 2048], P('tp'), may hold values from -0.125 to 0.125
- norm_gain: float32 [2048], replicated, may hold values from 0.1 to 1.9
- w_act: bfloat16 [2048, 5632], P('sp', 'tp'), may hold values from -0.125 to 0.125
- w_lin: bfloat16 [2048, 5632], P('sp', 'tp'), may hold values from -0.125 to 0.125
- conv_taps: float32 [2, 3, 5632], P(None, None, 'tp'), may hold values from -3.5 to 3.5
- w_down: bfloat16 [5632, 2048], P('tp', 'sp'), may hold values from -0.078125 to 0.078125
Outputs:
- layer_out: bfloat16 [32768, 2048], P(('sp', 'tp'))
The draws below stay inside these ranges and needn't reach their ends.
Inputs may be any that keep to these rules, and one draw needn't show every extreme that they name: `rate_real`: all entries negative. `damping`: all entries at most zero.
All inputs are finite; a program needn't handle non-finite values.
Results may differ from the reference program's by a relative error of at most 0.02.
Values may be sent and summed in bfloat16 or wider, within the bound.
A program may use at most 192 MiB of HBM per device.

```python
import math
import jax
import jax.numpy as jnp
from jax import lax

D = 2048
GROUP = 16
SSM_CLUSTERS = 128
STATE = 64
FF = 5632
CONV = 3
TOK_DEV = 512
SERIES_SPAN = 32768
N_TP = 4


def draw_rate_real(key, part):
    pick_key, fast_key, slow_key = jax.random.split(jax.random.fold_in(key, 11), 3)
    slow_share = 0.5
    slow_groups = jax.random.bernoulli(pick_key, slow_share, (SSM_CLUSTERS,))
    fast_rates = -jnp.exp(jax.random.uniform(fast_key, (SSM_CLUSTERS, STATE), jnp.float32, math.log(0.25), math.log(1.5)))
    slow_rates = -jnp.exp(jax.random.uniform(slow_key, (SSM_CLUSTERS, STATE), jnp.float32, 0.0, math.log(4.0))) / SERIES_SPAN
    return jnp.where(slow_groups[:, None], slow_rates, fast_rates)


def draw_damping(key, part):
    rate_key, spike_index_seed, amplitude_seed = jax.random.split(jax.random.fold_in(key, 23), 3)
    block_rates = jnp.exp(jax.random.uniform(rate_key, (SERIES_SPAN // TOK_DEV, SSM_CLUSTERS), jnp.float32, 0.0, math.log(4.0)))
    baseline_value = -0.2 * jnp.repeat(block_rates, TOK_DEV, axis=0) / SERIES_SPAN
    spike_indices = jax.random.randint(spike_index_seed, (2, SSM_CLUSTERS), 0, SERIES_SPAN)
    spike_falloffs = jnp.log(jax.random.uniform(amplitude_seed, (2, SSM_CLUSTERS), jnp.float32, 0.55, 0.8))
    element_indices = jnp.arange(SERIES_SPAN)[:, None]
    spike_occurrences = jnp.where(element_indices == spike_indices[0][None, :], spike_falloffs[0][None, :], 0.0)
    spike_occurrences = spike_occurrences + jnp.where(element_indices == spike_indices[1][None, :], spike_falloffs[1][None, :], 0.0)
    return (baseline_value + spike_occurrences).astype(jnp.float32)


def levels(stream_key, dims, pieces, smallest, high):
    loudness = 1.0
    for axis_at, parts in pieces:
        heights = jax.random.uniform(jax.random.fold_in(jax.random.fold_in(stream_key, 6), axis_at), (parts,), jnp.float32, smallest / len(pieces), high / len(pieces))
        loudness = loudness * jnp.repeat(jnp.exp(heights), dims[axis_at] // parts).reshape((-1,) + (1,) * (len(dims) - 1 - axis_at))
    return loudness


def scatter_about(rng, extent, spread, most, cuts=(), dtype=jnp.bfloat16):
    gain = levels(rng, extent, cuts, -0.22, 0.18) if cuts else 1.0
    values = jax.random.normal(rng, extent, jnp.float32) * spread * gain
    return jnp.minimum(jnp.maximum(values, -most), most).astype(dtype)


def setup_inputs(seed: int = 0) -> dict:
    keys = jax.random.split(jax.random.key(seed), 16)
    return {
        "mixer_input": scatter_about(keys[0], (SERIES_SPAN, D), 1.0, 6.0, ((0, 64), (1, 4))),
        "residual": scatter_about(keys[1], (SERIES_SPAN, D), 1.0, 6.0, ((0, 256),)),
        "log_step": jnp.clip(-3.9 + 1.6000001 * jax.random.uniform(keys[2], (SSM_CLUSTERS,), jnp.float32) ** levels(keys[2], (SSM_CLUSTERS,), ((0, 4),), -0.2, 0.2), -3.9, -2.3),
        "rate_real": draw_rate_real(jax.random.fold_in(keys[15], 71), 0),
        "rate_imag": jnp.clip(jnp.exp(math.log(30.0) - 2.7080502 * jax.random.uniform(keys[4], (SSM_CLUSTERS, STATE), jnp.float32) ** levels(keys[4], (SSM_CLUSTERS, STATE), ((0, 4),), -0.2, 0.2)), 2.0, 30.0),
        "damping": draw_damping(jax.random.fold_in(keys[15], 71), 0),
        "in_map": scatter_about(keys[6], (2, SSM_CLUSTERS, STATE, GROUP), (2 * GROUP) ** -0.5, 1.0, ((1, 4),), jnp.float32),
        "out_map": scatter_about(keys[7], (2, SSM_CLUSTERS, GROUP, STATE), STATE ** -0.5, 0.75, ((1, 4),), jnp.float32),
        "skip": scatter_about(keys[8], (D,), 0.5, 3.0, ((0, 4),), jnp.float32),
        "w_out": scatter_about(keys[9], (D, D), D ** -0.5, 0.125, ((0, 4),)),
        "norm_gain": jnp.clip(1.0 + 0.18 * jax.random.normal(keys[10], (D,), jnp.float32), 0.1, 1.9),
        "w_act": scatter_about(keys[11], (D, FF), D ** -0.5, 0.125, ((0, 64), (1, 4))),
        "w_lin": scatter_about(keys[12], (D, FF), D ** -0.5, 0.125, ((0, 64), (1, 4))),
        "conv_taps": scatter_about(keys[13], (2, CONV, FF), CONV ** -0.5, 3.5, ((2, 4),), jnp.float32),
        "w_down": scatter_about(keys[14], (FF, D), FF ** -0.5, 0.078125, ((0, 4), (1, 64))),
    }


def combine(earlier, later):
    a1r, a1i, b1r, b1i = earlier
    a2r, a2i, b2r, b2i = later
    return (a2r * a1r - a2i * a1i, a2r * a1i + a2i * a1r, a2r * b1r - a2i * b1i + b2r, a2r * b1i + a2i * b1r + b2i)

def one_group(packed):
    group_in, group_damp, bbar_re, bbar_im, log_rate, angle_step, cmap_re, cmap_im, skip_group = packed
    hi = lax.Precision.HIGHEST
    drive_re = jnp.dot(group_in, bbar_re.T, precision=hi)
    drive_im = jnp.dot(group_in, bbar_im.T, precision=hi)
    magnitude = jnp.exp(log_rate[None, :] + group_damp[:, None])
    trans_re = magnitude * jnp.cos(angle_step)[None, :]
    trans_im = magnitude * jnp.sin(angle_step)[None, :]
    scanned = lax.associative_scan(combine, (trans_re, trans_im, drive_re, drive_im), axis=0)
    state_re, state_im = (scanned[2], scanned[3])
    return jnp.dot(state_re, cmap_re.T, precision=hi) - jnp.dot(state_im, cmap_im.T, precision=hi) + skip_group[None, :] * group_in

def rounded_sum(total, partial_value):
    return total + lax.optimization_barrier(partial_value.astype(jnp.bfloat16)).astype(jnp.float32)

def reference(mixer_input, residual, log_step, rate_real, rate_imag, damping, in_map, out_map, skip, w_out, norm_gain, w_act, w_lin, conv_taps, w_down):
    seq_len = mixer_input.shape[0]
    step_size = jnp.exp(log_step)[:, None]
    log_rate = rate_real * step_size
    angle_step = rate_imag * step_size
    magnitude = jnp.exp(log_rate)
    abar_re = magnitude * jnp.cos(angle_step)
    abar_im = magnitude * jnp.sin(angle_step)
    denominator = rate_real * rate_real + rate_imag * rate_imag
    minus_one = abar_re - 1.0
    factor_re = (minus_one * rate_real + abar_im * rate_imag) / denominator
    factor_im = (abar_im * rate_real - minus_one * rate_imag) / denominator
    bbar_re = factor_re[..., None] * in_map[0] - factor_im[..., None] * in_map[1]
    bbar_im = factor_re[..., None] * in_map[1] + factor_im[..., None] * in_map[0]
    inputs = jnp.transpose(mixer_input.astype(jnp.float32).reshape(seq_len, SSM_CLUSTERS, GROUP), (1, 0, 2))
    outputs = lax.map(one_group, (inputs, damping.T, bbar_re, bbar_im, log_rate, angle_step, out_map[0], out_map[1], skip.reshape(SSM_CLUSTERS, GROUP)))
    mixed = jnp.transpose(outputs, (1, 0, 2)).reshape(seq_len, D)
    activated = jax.nn.gelu(mixed).astype(jnp.bfloat16)
    width_tp = D // N_TP
    projected = jnp.zeros((seq_len, D), jnp.float32)
    for shard in range(N_TP):
        window = slice(shard * width_tp, (shard + 1) * width_tp)
        partial_value = jnp.dot(activated[:, window], w_out[window], preferred_element_type=jnp.float32)
        projected = rounded_sum(projected, partial_value)
    stream = (residual.astype(jnp.float32) + projected).astype(jnp.bfloat16)
    stream_f = stream.astype(jnp.float32)
    normed = (stream_f * lax.rsqrt(lax.optimization_barrier(jnp.mean(stream_f * stream_f, axis=-1, keepdims=True)) + 1e-06) * norm_gain).astype(jnp.bfloat16)
    hidden_tp = FF // N_TP
    channel_sum = jnp.zeros((seq_len, D), jnp.float32)
    for shard in range(N_TP):
        window = slice(shard * hidden_tp, (shard + 1) * hidden_tp)
        act_pre = jnp.dot(normed, w_act[:, window], preferred_element_type=jnp.float32).astype(jnp.bfloat16)
        lin_pre = jnp.dot(normed, w_lin[:, window], preferred_element_type=jnp.float32).astype(jnp.bfloat16)
        padding = jnp.zeros((CONV - 1, hidden_tp), jnp.float32)
        act_pad = jnp.concatenate([padding, act_pre.astype(jnp.float32)], axis=0)
        lin_pad = jnp.concatenate([padding, lin_pre.astype(jnp.float32)], axis=0)
        act_conv = jnp.zeros((seq_len, hidden_tp), jnp.float32)
        lin_conv = jnp.zeros((seq_len, hidden_tp), jnp.float32)
        for offset in range(CONV):
            act_conv = act_conv + conv_taps[0, offset, window][None, :] * act_pad[offset:offset + seq_len]
            lin_conv = lin_conv + conv_taps[1, offset, window][None, :] * lin_pad[offset:offset + seq_len]
        hidden = (jax.nn.silu(act_conv) * lin_conv).astype(jnp.bfloat16)
        partial_value = jnp.dot(hidden, w_down[window], preferred_element_type=jnp.float32)
        channel_sum = rounded_sum(channel_sum, partial_value)
    return (stream.astype(jnp.float32) + channel_sum).astype(jnp.bfloat16)
```

```python
import functools

import jax
import jax.numpy as jnp
from jax import lax
from jax.experimental import pallas as pl
from jax.experimental.pallas import tpu as pltpu
from jax.sharding import Mesh
from jax.sharding import PartitionSpec as P

F32, BF16 = jnp.float32, jnp.bfloat16
NT = (((1,), (1,)), ((), ()))
TN = (((0,), (0,)), ((), ()))
Q, CH, PAIRS = 8, 64, 16
CONV = 3
SP = ("sp_0", "sp_1", "sp_2")
SP_TP = ("sp_0", "sp_1", "sp_2", "tp")

def iota(shape, dim):
    return lax.broadcasted_iota(jnp.int32, shape, dim)

def cmul(ar, ai, br, bi):
    return ar * br - ai * bi, ar * bi + ai * br

def split3(x):
    hi = x.astype(BF16)
    r = x - hi.astype(F32)
    mid = r.astype(BF16)
    lo = (r - mid.astype(F32)).astype(BF16)
    return hi, mid, lo

def block_swap(x):
    s = iota(x.shape, 1)
    g = iota(x.shape, 2) // 16
    for b in (4, 2, 1):
        sb, gb = (s // b) % 2, (g // b) % 2
        down = pltpu.roll(pltpu.roll(x, 16 * b, axis=2), 8 - b, axis=1)
        if b == 4:
            up = down
        else:
            up = pltpu.roll(pltpu.roll(x, 128 - 16 * b, axis=2), b, axis=1)
        x = jnp.where(sb == gb, x, jnp.where(sb == 0, down, up))
    return x

def paired(even, odd):
    return jnp.concatenate([even, odd], axis=1)


def mixer_phase(r, comm, hooks=None):
    def rows(ref):
        return paired(ref[pl.ds(0, PAIRS, stride=2), :], ref[pl.ds(1, PAIRS, stride=2), :])

    rr, ri = rows(r.rr), rows(r.ri)
    step = jnp.exp(rows(r.ls))
    lr, th = rr * step, ri * step
    cos, sin = jnp.cos(th), jnp.sin(th)
    mag, inv = jnp.exp(lr), jnp.exp(-lr)
    ar, ai = mag * cos, mag * sin
    den = rr * rr + ri * ri
    r.fac[0] = ((ar - 1.0) * rr + ai * ri) / den
    r.fac[1] = (ai * rr - (ar - 1.0) * ri) / den
    one, zero = jnp.ones_like(ar), jnp.zeros_like(ar)
    pr, pi, nr, ni = one, zero, one, zero
    for s in range(Q):
        at = pl.ds(s, PAIRS, stride=Q)
        r.pw[0, at, :], r.pw[1, at, :] = nr, ni
        r.pw[2, at, :], r.pw[3, at, :] = pr, pi
        pr, pi = cmul(pr, pi, ar, ai)
        nr, ni = cmul(nr, ni, inv * cos, -inv * sin)
    d = r.damp[...]
    lane = iota(d.shape, 1) % Q
    for sh in (1, 2, 4):
        d = d + jnp.where(lane >= sh, pltpu.roll(d, sh, axis=1), 0.0)
    ex = (iota((96, 512), 0) % 32 == iota((96, 512), 1) // 16).astype(F32).astype(BF16)
    for n, sign in enumerate((-1.0, 1.0)):
        parts = jnp.concatenate([p.astype(F32) for p in split3(jnp.exp(sign * d))], axis=0).astype(BF16)
        r.ex[n] = lax.dot_general(parts, ex, TN, preferred_element_type=F32)
    pick = (iota((CH, 512), 1) == Q * iota((CH, 512), 0) + Q - 1).astype(F32).astype(BF16)
    ends = sum(lax.dot_general(pick, p, NT, preferred_element_type=F32) for p in split3(d))
    ends = jnp.exp(ends)
    low = iota((CH, 128), 1) < 64
    for k in range(PAIRS):
        r.e7[pl.ds(k, CH, stride=PAIRS), :] = jnp.where(low, ends[:, 2 * k : 2 * k + 1], ends[:, 2 * k + 1 : 2 * k + 2])

    def spread(b, _):
        j, c = b // 8, b % 8
        at = pl.ds(pl.multiple_of(c * 64, 64), 64)
        lanes = pl.ds(pl.multiple_of(j * 128, 128), 128)
        v = r.u[at, lanes].astype(F32) * r.ex[0, at, lanes]
        r.z[pl.ds(pl.multiple_of(b * 64, 64), 64), :] = block_swap(v.reshape(8, 8, 128)).reshape(64, 128)
        return 0

    lax.fori_loop(0, 32, spread, 0)

    def group_rows(k):
        first = (k // 4) * 512 + (k % 4) * 2
        return pl.ds(first, CH, stride=8), pl.ds(first + 1, CH, stride=8)

    low = iota((128, 128), 1) < 64

    def stacked(re, im):
        top = jnp.concatenate([jnp.where(low, re, 0.0), jnp.where(low, im, 0.0)], axis=1)
        bottom = jnp.concatenate([jnp.where(low, 0.0, re), jnp.where(low, 0.0, im)], axis=1)
        return jnp.concatenate([top, bottom], axis=0).astype(BF16)

    def outer(which, k, br, bi):
        at = pl.ds(pl.multiple_of(k * Q, Q), Q)
        wr, wi = r.pw[which, at, :][:, None, :], r.pw[which + 1, at, :][:, None, :]
        br, bi = br[None], bi[None]
        re, im = cmul(wr, wi, br, bi)
        return re.reshape(128, 128), im.reshape(128, 128)

    def inputs_of(k):
        even, odd = group_rows(k)
        return jnp.concatenate([r.z[even, :], r.z[odd, :]], axis=1).astype(BF16)

    def states_in(k, _):
        br, bi = paired(r.inm[0, 2 * k], r.inm[0, 2 * k + 1]), paired(r.inm[1, 2 * k], r.inm[1, 2 * k + 1])
        br, bi = cmul(r.fac[0, pl.ds(k, 1), :], r.fac[1, pl.ds(k, 1), :], br, bi)
        p = stacked(*outer(0, k, br, bi))
        r.pb[k] = p
        s = jnp.dot(inputs_of(k), p, preferred_element_type=F32)
        at = pl.ds(k, CH, stride=PAIRS)
        r.sr[at, :] = s[:, :128]
        r.si[at, :] = s[:, 128:]
        return 0

    lax.fori_loop(0, PAIRS, states_in, 0, unroll=2)

    a2r, a2i = cmul(ar, ai, ar, ai)
    a4r, a4i = cmul(a2r, a2i, a2r, a2i)
    a8r, a8i = cmul(a4r, a4i, a4r, a4i)

    def advance(c, carry, keep):
        vr, vi, e_all = carry
        at = pl.ds(pl.multiple_of(c * PAIRS, PAIRS), PAIRS)
        e = r.e7[at, :]
        tr, ti = (vr + r.sr[at, :]) * e, (vi + r.si[at, :]) * e
        if keep:
            r.sr[at, :], r.si[at, :] = vr, vi
        vr, vi = cmul(a8r, a8i, tr, ti)
        return vr, vi, e_all * e

    vr, vi, e_all = lax.fori_loop(0, CH, functools.partial(advance, keep=False), (zero, zero, one), unroll=8)

    causal = (iota((256, 256), 0) // 16) % Q <= (iota((256, 256), 1) // 16) % Q

    def inside(k, _):
        cr, ci = paired(r.outm[0, 2 * k], r.outm[0, 2 * k + 1]), paired(r.outm[1, 2 * k], r.outm[1, 2 * k + 1])
        qr, qi = outer(2, k, cr, ci)
        q = stacked(qr, -qi)
        r.qb[k] = q
        m = lax.dot_general(r.pb[k], q, NT, preferred_element_type=F32)
        m = jnp.where(causal, m, 0.0).astype(BF16)
        out = jnp.dot(inputs_of(k), m, preferred_element_type=F32)
        even, odd = group_rows(k)
        r.y[even, :] = out[:, :128]
        r.y[odd, :] = out[:, 128:]
        return 0

    def inside_part(n):
        cuts = (0, 6, 12, 16)
        lax.fori_loop(cuts[n], cuts[n + 1], inside, 0, unroll=2)

    vr, vi = comm(ar, ai, vr, vi, e_all, inside_part)
    lax.fori_loop(0, CH, functools.partial(advance, keep=True), (vr, vi, one), unroll=8)

    def outputs(k, _):
        at = pl.ds(k, CH, stride=PAIRS)
        v = jnp.concatenate([r.sr[at, :], r.si[at, :]], axis=1).astype(BF16)
        out = lax.dot_general(v, r.qb[k], NT, preferred_element_type=F32)
        even, odd = group_rows(k)
        r.y[even, :] += out[:, :128]
        r.y[odd, :] += out[:, 128:]
        return 0

    lax.fori_loop(0, PAIRS, outputs, 0, unroll=2)

    def finish(b, _):
        j, c = b // 8, b % 8
        at = pl.ds(pl.multiple_of(c * 64, 64), 64)
        lanes = pl.ds(pl.multiple_of(j * 128, 128), 128)
        v = r.y[pl.ds(pl.multiple_of(b * 64, 64), 64), :]
        v = block_swap(v.reshape(8, 8, 128)).reshape(64, 128)
        mixed = v * r.ex[1, at, lanes] + r.skip[:, lanes] * r.u[at, lanes].astype(F32)
        r.act[at, lanes] = jax.nn.gelu(mixed).astype(BF16)
        return 0

    lax.fori_loop(0, 32, finish, 0)


def fold(acc, vr, vi, e, wr, wi, use):
    er, ei = cmul(wr * e, wi * e, acc[0], acc[1])
    return jnp.where(use, er + vr, acc[0]), jnp.where(use, ei + vi, acc[1]), jnp.where(use, acc[2] * e, acc[2])


def squared(w, times):
    for _ in range(times):
        w = cmul(*w, *w)
    return w


class Refs:
    def __init__(self, **named):
        self.__dict__.update(named)


MIXER_SCRATCH = dict(
    fac=pltpu.VMEM((2, PAIRS, 128), F32), pw=pltpu.VMEM((4, PAIRS * Q, 128), F32), ex=pltpu.VMEM((2, 512, 512), F32),
    e7=pltpu.VMEM((CH * PAIRS, 128), F32), z=pltpu.VMEM((2048, 128), F32), y=pltpu.VMEM((2048, 128), F32),
    pb=pltpu.VMEM((PAIRS, 256, 256), BF16), qb=pltpu.VMEM((PAIRS, 256, 256), BF16),
    sr=pltpu.VMEM((CH * PAIRS, 128), F32), si=pltpu.VMEM((CH * PAIRS, 128), F32),
)


EXCHANGE_SCRATCH = dict(
    mine=pltpu.VMEM((3, 3, PAIRS, 128), F32), got_c=pltpu.VMEM((1, 3, PAIRS, 128), F32), got_x=pltpu.VMEM((3, 3, PAIRS, 128), F32),
    got_z=pltpu.VMEM((7, 3, PAIRS, 128), F32), ssem=pltpu.SemaphoreType.DMA((11,)), rsem=pltpu.SemaphoreType.DMA((11,)),
)


def greet(groups):
    barrier = pltpu.get_barrier_semaphore()
    many = 0
    for axis, count in groups:
        me = lax.axis_index(axis)
        for d in range(1, count):
            pl.semaphore_signal(barrier, inc=1, device_id={axis: lax.rem(me + d, count)}, device_id_type=pl.DeviceIdType.MESH)
            many += 1
    pl.semaphore_wait(barrier, many)


def exchange(r, ar, ai, vr, vi, e, part):
    core, x, z = lax.axis_index("sp_2"), lax.axis_index("sp_1"), lax.axis_index("sp_0")

    def copies(level, axis, me, count, got, first):
        return [
            pltpu.make_async_remote_copy(
                src_ref=r.mine.at[level], dst_ref=got.at[d - 1], send_sem=r.ssem.at[first + d - 1], recv_sem=r.rsem.at[first + d - 1],
                device_id={axis: lax.rem(me + d, count)}, device_id_type=pl.DeviceIdType.MESH,
            )
            for d in range(1, count)
        ]

    def put(level, parts):
        for n, v in enumerate(parts):
            r.mine[level, n] = v

    def of(got, slot):
        return got[slot, 0], got[slot, 1], got[slot, 2]

    nothing = (jnp.zeros_like(vr), jnp.zeros_like(vr), jnp.ones_like(vr))
    w1 = squared((ar, ai), 9)
    w2 = squared(w1, 1)
    w8 = squared(w2, 2)
    own = (vr, vi, e)
    put(0, own)
    for c in copies(0, "sp_2", core, 2, r.got_c, 0):
        c.start()
    part(0)
    for c in copies(0, "sp_2", core, 2, r.got_c, 0):
        c.wait()
    other = of(r.got_c, 0)
    early = [jnp.where(core == 0, a, b) for a, b in zip(own, other)]
    late = [jnp.where(core == 0, b, a) for a, b in zip(own, other)]
    chip = fold(early, *late, *w1, True)
    put(1, chip)
    for c in copies(1, "sp_1", x, 4, r.got_x, 1):
        c.start()
    part(1)
    for c in copies(1, "sp_1", x, 4, r.got_x, 1):
        c.wait()
    total = nothing
    for d in (3, 2, 1):
        total = fold(total, *of(r.got_x, d - 1), *w2, d <= x)
    total = fold(total, *chip, *w2, True)
    for d in (3, 2, 1):
        total = fold(total, *of(r.got_x, d - 1), *w2, d > x)
    put(2, total)
    sends = copies(2, "sp_0", z, 8, r.got_z, 4)
    for d in range(1, 8):
        pl.when(z + d < 8)(sends[d - 1].start)
    part(2)
    for d in range(1, 8):
        pl.when(z + d < 8)(sends[d - 1].wait_send)
        pl.when(z >= d)(sends[d - 1].wait_recv)
    enter = nothing
    for d in range(7, 0, -1):
        enter = fold(enter, *of(r.got_z, d - 1), *w8, d <= z)
    for d in (3, 2, 1):
        enter = fold(enter, *of(r.got_x, d - 1), *w2, d <= x)
    enter = fold(enter, *other, *w1, core == 1)
    return enter[0], enter[1]

SCRATCH = {**MIXER_SCRATCH, **EXCHANGE_SCRATCH}


def mixer_kernel(u, damp, ls, rr, ri, inm, outm, skip, act, *scratch):
    r = Refs(u=u, damp=damp, ls=ls, rr=rr, ri=ri, inm=inm, outm=outm, skip=skip, act=act, **dict(zip(SCRATCH, scratch)))
    r.got_z[...] = jnp.zeros_like(r.got_z)
    greet((("sp_2", 2), ("sp_1", 4), ("sp_0", 8)))
    mixer_phase(r, functools.partial(exchange, r))


def mixer(mixer_input, log_step, rate_real, rate_imag, damping, in_map, out_map, skip):
    return pl.pallas_call(
        mixer_kernel,
        out_shape=jax.ShapeDtypeStruct(mixer_input.shape, BF16),
        in_specs=[pl.BlockSpec(memory_space=pltpu.VMEM)] * 8,
        out_specs=pl.BlockSpec(memory_space=pltpu.VMEM),
        scratch_shapes=list(SCRATCH.values()),
        compiler_params=pltpu.CompilerParams(collective_id=0, has_side_effects=True, vmem_limit_bytes=40 * 2**20),
        cost_estimate=pl.CostEstimate(flops=6 * 10**9, bytes_accessed=4 * 10**6, transcendentals=0),
        name="mixer",
    )(
        mixer_input, damping.T, jnp.broadcast_to(log_step[:, None], rate_real.shape), rate_real, rate_imag,
        in_map.transpose(0, 1, 3, 2), out_map, skip[None],
    )


def sent_together(arrays, axis, dim, along):
    widths = [a.shape[along] for a in arrays]
    both = jnp.concatenate(arrays, axis=along)
    result = lax.all_gather(both, axis, axis=dim, tiled=True)
    return tuple(jnp.split(result, [sum(widths[:k]) for k in range(1, len(widths))], axis=along))


def cut_along(array, dim, peers):
    before, after = (array.shape[:dim], array.shape[dim + 1 :])
    return jnp.moveaxis(array.reshape(*before, peers, -1, *after), dim, 0)


def sent_and_summed(array, axis, dim):
    parts = cut_along(array, dim, lax.axis_size(axis))
    arrived = lax.all_to_all(parts, axis, split_axis=0, concat_axis=0, tiled=True)
    return arrived.astype(jnp.float32).sum(axis=0)


def joined_along(parts, dim):
    shape = list(parts.shape[1:])
    shape[dim] *= parts.shape[0]
    return jnp.moveaxis(parts, 0, dim).reshape(shape)


def from_everyone(array, axis):
    copies = jnp.broadcast_to(array, (lax.axis_size(axis), *array.shape))
    return lax.all_to_all(copies, axis, split_axis=0, concat_axis=0, tiled=True)


def collect(array, axis, dim):
    return joined_along(from_everyone(array, axis), dim)


def from_behind(value, axis, steps):
    count = lax.axis_size(axis)
    initial, last = (max(0, -steps), min(count, count - steps))
    return lax.ppermute(value, axis, [(source, source + steps) for source in range(initial, last)])


def normalize(stream, norm_gain):
    stream_f = stream.astype(jnp.float32)
    scale = lax.rsqrt(jnp.mean(stream_f * stream_f, axis=-1, keepdims=True) + 1e-06)
    return (stream_f * scale * norm_gain).astype(jnp.bfloat16)


def causal_conv(act_pre, lin_pre, previous, taps):
    row_count, width = act_pre.shape
    act_pad = jnp.concatenate([previous[0], act_pre], axis=0).astype(jnp.float32)
    lin_pad = jnp.concatenate([previous[1], lin_pre], axis=0).astype(jnp.float32)
    act_conv = jnp.zeros((row_count, width), jnp.float32)
    lin_conv = jnp.zeros((row_count, width), jnp.float32)
    for offset in range(CONV):
        act_conv = act_conv + taps[0, offset][None, :] * act_pad[offset : offset + row_count]
        lin_conv = lin_conv + taps[1, offset][None, :] * lin_pad[offset : offset + row_count]
    return (jax.nn.silu(act_conv) * lin_conv).astype(jnp.bfloat16)


def per_device(
    mixer_input,
    residual,
    log_step,
    rate_real,
    rate_imag,
    damping,
    in_map,
    out_map,
    skip,
    w_out,
    norm_gain,
    w_act,
    w_lin,
    conv_taps,
    w_down,
):
    tokens_here = mixer_input.shape[0]
    act_full, lin_full = sent_together((w_act, w_lin), SP, 0, 1)
    down_full = lax.all_gather(w_down, SP, axis=1, tiled=True)
    activated = mixer(mixer_input, log_step, rate_real, rate_imag, damping, in_map, out_map, skip)
    block = activated
    projected = sent_and_summed(
        jnp.dot(block, w_out, preferred_element_type=jnp.float32).astype(jnp.bfloat16), "tp", 0
    )
    stream = (residual.astype(jnp.float32) + projected).astype(jnp.bfloat16)
    normed_all = collect(normalize(stream, norm_gain), "tp", 0)
    act_pre = jnp.dot(normed_all, act_full, preferred_element_type=jnp.float32).astype(jnp.bfloat16)
    lin_pre = jnp.dot(normed_all, lin_full, preferred_element_type=jnp.float32).astype(jnp.bfloat16)
    edge = tokens_here - (CONV - 1)
    previous = from_behind((act_pre[edge:], lin_pre[edge:]), SP, 1)
    hidden = causal_conv(act_pre, lin_pre, previous, conv_taps)
    block = hidden
    channel_sum = sent_and_summed(
        jnp.dot(block, down_full, preferred_element_type=jnp.float32).astype(jnp.bfloat16), "tp", 0
    )
    return (stream.astype(jnp.float32) + channel_sum).astype(jnp.bfloat16)


def solution(mesh):
    split = Mesh(mesh.devices.reshape(8, 4, 2, mesh.shape["tp"]), ("sp_0", "sp_1", "sp_2", "tp"))
    in_specs = (
        P(SP, "tp"),
        P(SP_TP, None),
        P("tp"),
        P("tp", None),
        P("tp", None),
        P(SP, "tp"),
        P(None, "tp", None, None),
        P(None, "tp", None, None),
        P("tp"),
        P("tp", None),
        P(),
        P(SP, "tp"),
        P(SP, "tp"),
        P(None, None, "tp"),
        P("tp", SP),
    )
    out_specs = P(SP_TP, None)
    return jax.shard_map(
        per_device, mesh=split, in_specs=in_specs, out_specs=out_specs, check_vma=False
    )
```

```python
import functools

import jax
import jax.numpy as jnp
from jax import lax
from jax.experimental import pallas as pl
from jax.experimental.pallas import tpu as pltpu
from jax.sharding import Mesh
from jax.sharding import PartitionSpec as P

F32, BF16 = jnp.float32, jnp.bfloat16
NT = (((1,), (1,)), ((), ()))
TN = (((0,), (0,)), ((), ()))
Q, CH, PAIRS = 8, 64, 16
SP = ("sp_0", "sp_1", "sp_2")
SP_TP = ("sp_0", "sp_1", "sp_2", "tp")
MESH = pl.DeviceIdType.MESH

def iota(shape, dim):
    return lax.broadcasted_iota(jnp.int32, shape, dim)

def cmul(ar, ai, br, bi):
    return ar * br - ai * bi, ar * bi + ai * br

def split3(x):
    hi = x.astype(BF16)
    r = x - hi.astype(F32)
    mid = r.astype(BF16)
    lo = (r - mid.astype(F32)).astype(BF16)
    return hi, mid, lo

def block_swap(x):
    s = iota(x.shape, 1)
    g = iota(x.shape, 2) // 16
    for b in (4, 2, 1):
        sb, gb = (s // b) % 2, (g // b) % 2
        down = pltpu.roll(pltpu.roll(x, 16 * b, axis=2), 8 - b, axis=1)
        if b == 4:
            up = down
        else:
            up = pltpu.roll(pltpu.roll(x, 128 - 16 * b, axis=2), b, axis=1)
        x = jnp.where(sb == gb, x, jnp.where(sb == 0, down, up))
    return x

def paired(even, odd):
    return jnp.concatenate([even, odd], axis=1)


def mixer_phase(r, comm, at_point):
    def rows(ref):
        return paired(ref[pl.ds(0, PAIRS, stride=2), :], ref[pl.ds(1, PAIRS, stride=2), :])

    rr, ri = rows(r.rr), rows(r.ri)
    step = jnp.exp(rows(r.ls))
    lr, th = rr * step, ri * step
    cos, sin = jnp.cos(th), jnp.sin(th)
    mag, inv = jnp.exp(lr), jnp.exp(-lr)
    ar, ai = mag * cos, mag * sin
    den = rr * rr + ri * ri
    r.fac[0] = ((ar - 1.0) * rr + ai * ri) / den
    r.fac[1] = (ai * rr - (ar - 1.0) * ri) / den
    one, zero = jnp.ones_like(ar), jnp.zeros_like(ar)
    pr, pi, nr, ni = one, zero, one, zero
    for s in range(Q):
        at = pl.ds(s, PAIRS, stride=Q)
        r.pw[0, at, :], r.pw[1, at, :] = nr, ni
        r.pw[2, at, :], r.pw[3, at, :] = pr, pi
        pr, pi = cmul(pr, pi, ar, ai)
        nr, ni = cmul(nr, ni, inv * cos, -inv * sin)
    d = r.damp[...]
    lane = iota(d.shape, 1) % Q
    for sh in (1, 2, 4):
        d = d + jnp.where(lane >= sh, pltpu.roll(d, sh, axis=1), 0.0)
    ex = (iota((96, 512), 0) % 32 == iota((96, 512), 1) // 16).astype(F32).astype(BF16)
    for n, sign in enumerate((-1.0, 1.0)):
        parts = jnp.concatenate([p.astype(F32) for p in split3(jnp.exp(sign * d))], axis=0).astype(BF16)
        r.ex[n] = lax.dot_general(parts, ex, TN, preferred_element_type=F32)
    pick = (iota((CH, 512), 1) == Q * iota((CH, 512), 0) + Q - 1).astype(F32).astype(BF16)
    ends = sum(lax.dot_general(pick, p, NT, preferred_element_type=F32) for p in split3(d))
    ends = jnp.exp(ends)
    low = iota((CH, 128), 1) < 64
    for k in range(PAIRS):
        r.e7[pl.ds(k, CH, stride=PAIRS), :] = jnp.where(low, ends[:, 2 * k : 2 * k + 1], ends[:, 2 * k + 1 : 2 * k + 2])

    at_point(0)

    def spread(b, _):
        j, c = b // 8, b % 8
        at = pl.ds(pl.multiple_of(c * 64, 64), 64)
        lanes = pl.ds(pl.multiple_of(j * 128, 128), 128)
        v = r.u[at, lanes].astype(F32) * r.ex[0, at, lanes]
        r.z[pl.ds(pl.multiple_of(b * 64, 64), 64), :] = block_swap(v.reshape(8, 8, 128)).reshape(64, 128)
        return 0

    lax.fori_loop(0, 32, spread, 0)
    at_point(1)

    def group_rows(k):
        first = (k // 4) * 512 + (k % 4) * 2
        return pl.ds(first, CH, stride=8), pl.ds(first + 1, CH, stride=8)

    low = iota((128, 128), 1) < 64

    def stacked(re, im):
        top = jnp.concatenate([jnp.where(low, re, 0.0), jnp.where(low, im, 0.0)], axis=1)
        bottom = jnp.concatenate([jnp.where(low, 0.0, re), jnp.where(low, 0.0, im)], axis=1)
        return jnp.concatenate([top, bottom], axis=0).astype(BF16)

    def outer(which, k, br, bi):
        at = pl.ds(pl.multiple_of(k * Q, Q), Q)
        wr, wi = r.pw[which, at, :][:, None, :], r.pw[which + 1, at, :][:, None, :]
        br, bi = br[None], bi[None]
        re, im = cmul(wr, wi, br, bi)
        return re.reshape(128, 128), im.reshape(128, 128)

    def inputs_of(k):
        even, odd = group_rows(k)
        return jnp.concatenate([r.z[even, :], r.z[odd, :]], axis=1).astype(BF16)

    def states_in(k, _):
        br, bi = paired(r.inm[0, 2 * k], r.inm[0, 2 * k + 1]), paired(r.inm[1, 2 * k], r.inm[1, 2 * k + 1])
        br, bi = cmul(r.fac[0, pl.ds(k, 1), :], r.fac[1, pl.ds(k, 1), :], br, bi)
        p = stacked(*outer(0, k, br, bi))
        r.pb[k] = p
        s = jnp.dot(inputs_of(k), p, preferred_element_type=F32)
        at = pl.ds(k, CH, stride=PAIRS)
        r.sr[at, :] = s[:, :128]
        r.si[at, :] = s[:, 128:]
        return 0

    lax.fori_loop(0, 8, states_in, 0, unroll=2)
    at_point(2)
    lax.fori_loop(8, PAIRS, states_in, 0, unroll=2)
    at_point(3)

    a2r, a2i = cmul(ar, ai, ar, ai)
    a4r, a4i = cmul(a2r, a2i, a2r, a2i)
    a8r, a8i = cmul(a4r, a4i, a4r, a4i)

    def advance(c, carry, keep):
        vr, vi, e_all = carry
        at = pl.ds(pl.multiple_of(c * PAIRS, PAIRS), PAIRS)
        e = r.e7[at, :]
        tr, ti = (vr + r.sr[at, :]) * e, (vi + r.si[at, :]) * e
        if keep:
            r.sr[at, :], r.si[at, :] = vr, vi
        vr, vi = cmul(a8r, a8i, tr, ti)
        return vr, vi, e_all * e

    vr, vi, e_all = lax.fori_loop(0, CH, functools.partial(advance, keep=False), (zero, zero, one), unroll=8)

    causal = (iota((256, 256), 0) // 16) % Q <= (iota((256, 256), 1) // 16) % Q

    def inside(k, _):
        cr, ci = paired(r.outm[0, 2 * k], r.outm[0, 2 * k + 1]), paired(r.outm[1, 2 * k], r.outm[1, 2 * k + 1])
        qr, qi = outer(2, k, cr, ci)
        q = stacked(qr, -qi)
        r.qb[k] = q
        m = lax.dot_general(r.pb[k], q, NT, preferred_element_type=F32)
        m = jnp.where(causal, m, 0.0).astype(BF16)
        out = jnp.dot(inputs_of(k), m, preferred_element_type=F32)
        even, odd = group_rows(k)
        r.y[even, :] = out[:, :128]
        r.y[odd, :] = out[:, 128:]
        return 0

    def inside_part(n):
        cuts = (0, 6, 12, 16)
        lax.fori_loop(cuts[n], cuts[n + 1], inside, 0, unroll=2)

    vr, vi = comm(ar, ai, vr, vi, e_all, inside_part)
    lax.fori_loop(0, CH, functools.partial(advance, keep=True), (vr, vi, one), unroll=8)
    at_point(4)

    def outputs(k, _):
        at = pl.ds(k, CH, stride=PAIRS)
        v = jnp.concatenate([r.sr[at, :], r.si[at, :]], axis=1).astype(BF16)
        out = lax.dot_general(v, r.qb[k], NT, preferred_element_type=F32)
        even, odd = group_rows(k)
        r.y[even, :] += out[:, :128]
        r.y[odd, :] += out[:, 128:]
        return 0

    lax.fori_loop(0, PAIRS, outputs, 0, unroll=2)
    at_point(5)

    def finish(first, b, _):
        j, c = b // 2, first + b % 2
        at = pl.ds(pl.multiple_of(c * 64, 64), 64)
        lanes = pl.ds(pl.multiple_of(j * 128, 128), 128)
        v = r.y[pl.ds(pl.multiple_of(j * 512 + c * 64, 64), 64), :]
        v = block_swap(v.reshape(8, 8, 128)).reshape(64, 128)
        mixed = v * r.ex[1, at, lanes] + r.skip[:, lanes] * r.u[at, lanes].astype(F32)
        r.act[at, lanes] = jax.nn.gelu(mixed).astype(BF16)
        return 0

    me = lax.axis_index("tp")
    for d in (2, 1, 3, 0):
        q = lax.rem(me + d, 4)
        lax.fori_loop(0, 8, functools.partial(finish, 2 * q), 0)
        if d:
            to_rows(r, d).start()
        else:
            r.acts[me] = r.act[pl.ds(pl.multiple_of(me * 128, 128), 128), :]


def fold(acc, vr, vi, e, wr, wi, use):
    er, ei = cmul(wr * e, wi * e, acc[0], acc[1])
    return jnp.where(use, er + vr, acc[0]), jnp.where(use, ei + vi, acc[1]), jnp.where(use, acc[2] * e, acc[2])


def squared(w, times):
    for _ in range(times):
        w = cmul(*w, *w)
    return w


class Refs:
    def __init__(self, **named):
        self.__dict__.update(named)


MIXER_SCRATCH = dict(
    fac=pltpu.VMEM((2, PAIRS, 128), F32), pw=pltpu.VMEM((4, PAIRS * Q, 128), F32), ex=pltpu.VMEM((2, 512, 512), F32),
    e7=pltpu.VMEM((CH * PAIRS, 128), F32), z=pltpu.VMEM((2048, 128), F32), y=pltpu.VMEM((2048, 128), F32),
    pb=pltpu.VMEM((PAIRS, 256, 256), BF16), qb=pltpu.VMEM((PAIRS, 256, 256), BF16),
    sr=pltpu.VMEM((CH * PAIRS, 128), F32), si=pltpu.VMEM((CH * PAIRS, 128), F32),
)


EXCHANGE_SCRATCH = dict(
    mine=pltpu.VMEM((3, 3, PAIRS, 128), F32), got_c=pltpu.VMEM((1, 3, PAIRS, 128), F32), got_x=pltpu.VMEM((3, 3, PAIRS, 128), F32),
    got_z=pltpu.VMEM((7, 3, PAIRS, 128), F32), ssem=pltpu.SemaphoreType.DMA((11,)), rsem=pltpu.SemaphoreType.DMA((11,)),
)


def greet(groups, others):
    barrier = pltpu.get_barrier_semaphore()
    peers = [{axis: lax.rem(lax.axis_index(axis) + d, count)} for axis, count in groups for d in range(1, count)] + others
    for peer in peers:
        pl.semaphore_signal(barrier, inc=1, device_id=peer, device_id_type=MESH)
    pl.semaphore_wait(barrier, len(peers))


def exchange(r, between, ar, ai, vr, vi, e, part):
    core, x, z = lax.axis_index("sp_2"), lax.axis_index("sp_1"), lax.axis_index("sp_0")

    def copies(level, axis, me, count, got, first):
        return [
            pltpu.make_async_remote_copy(
                src_ref=r.mine.at[level], dst_ref=got.at[d - 1], send_sem=r.ssem.at[first + d - 1], recv_sem=r.rsem.at[first + d - 1],
                device_id={axis: lax.rem(me + d, count)}, device_id_type=MESH,
            )
            for d in range(1, count)
        ]

    def put(level, parts):
        for n, v in enumerate(parts):
            r.mine[level, n] = v

    def of(got, slot):
        return got[slot, 0], got[slot, 1], got[slot, 2]

    nothing = (jnp.zeros_like(vr), jnp.zeros_like(vr), jnp.ones_like(vr))
    w1 = squared((ar, ai), 9)
    w2 = squared(w1, 1)
    w8 = squared(w2, 2)
    own = (vr, vi, e)
    put(0, own)
    for c in copies(0, "sp_2", core, 2, r.got_c, 0):
        c.start()
    part(0)
    for c in copies(0, "sp_2", core, 2, r.got_c, 0):
        c.wait()
    other = of(r.got_c, 0)
    early = [jnp.where(core == 0, a, b) for a, b in zip(own, other)]
    late = [jnp.where(core == 0, b, a) for a, b in zip(own, other)]
    chip = fold(early, *late, *w1, True)
    put(1, chip)
    for c in copies(1, "sp_1", x, 4, r.got_x, 1):
        c.start()
    part(1)
    for c in copies(1, "sp_1", x, 4, r.got_x, 1):
        c.wait()
    total = nothing
    for d in (3, 2, 1):
        total = fold(total, *of(r.got_x, d - 1), *w2, d <= x)
    total = fold(total, *chip, *w2, True)
    for d in (3, 2, 1):
        total = fold(total, *of(r.got_x, d - 1), *w2, d > x)
    put(2, total)
    sends = copies(2, "sp_0", z, 8, r.got_z, 4)
    for d in range(1, 8):
        pl.when(z + d < 8)(sends[d - 1].start)
    between()
    part(2)
    for d in range(1, 8):
        pl.when(z + d < 8)(sends[d - 1].wait_send)
        pl.when(z >= d)(sends[d - 1].wait_recv)
    enter = nothing
    for d in range(7, 0, -1):
        enter = fold(enter, *of(r.got_z, d - 1), *w8, d <= z)
    for d in (3, 2, 1):
        enter = fold(enter, *of(r.got_x, d - 1), *w2, d <= x)
    enter = fold(enter, *other, *w1, core == 1)
    return enter[0], enter[1]

def to_rows(r, d):
    me = lax.axis_index("tp")
    q = lax.rem(me + d, 4)
    return pltpu.make_async_remote_copy(
        src_ref=r.act.at[pl.ds(pl.multiple_of(q * 128, 128), 128), :], dst_ref=r.acts.at[me],
        send_sem=r.rows_s.at[d - 1], recv_sem=r.rows_r.at[d - 1], device_id={"tp": q}, device_id_type=MESH,
    )


class Ring:
    def __init__(self, axis, count, chunk, ssem, rsem, shared=None):
        self.axis, self.count, self.chunk, self.ssem, self.rsem, self.shared = axis, count, chunk, ssem, rsem, shared
        self.me, self.half = lax.axis_index(axis), count // 2

    def place(self, steps):
        return lax.rem(self.me + steps + self.count, self.count)

    def copy(self, step, way, k, owner):
        n = ((step - 1) * 2 + way) * 2 + k
        sign = 1 - 2 * way
        ref = self.chunk(self.place(owner), k)
        return pltpu.make_async_remote_copy(
            src_ref=ref, dst_ref=ref, send_sem=self.ssem.at[n], recv_sem=self.rsem.at[n],
            device_id={self.axis: self.place(sign)}, device_id_type=MESH,
        )

    def sends(self, step, i):
        return [self.copy(step, way, (i, 1 - i)[way], -(1 - 2 * way) * (step - 1)) for way in (0, 1)]

    def begin(self):
        for i in (0, 1):
            for c in self.sends(1, i):
                c.start()

    def services(self):
        return [(s, i) for s in range(1, self.half + 1) for i in (0, 1) if s < self.half or i == 0]

    def partner_copy(self, step, way, k, core):
        n = ((step - 1) * 2 + way) * 2 + k
        ref = self.chunk(self.place(-(1 - 2 * way) * step), k, core)
        me = lax.axis_index("sp_2")
        return pltpu.make_async_remote_copy(
            src_ref=ref, dst_ref=ref, send_sem=self.shared[0].at[n], recv_sem=self.shared[1].at[n],
            device_id={"sp_2": 1 - me}, device_id_type=MESH,
        )

    def service(self, step, i):
        for way in (0, 1):
            k = (i, 1 - i)[way]
            self.copy(step, way, k, -(1 - 2 * way) * step).wait_recv()
            if step + 1 < self.half or (step + 1 == self.half and i == 0):
                self.copy(step + 1, way, k, -(1 - 2 * way) * step).start()
            if self.shared:
                self.partner_copy(step, way, k, lax.axis_index("sp_2")).start()

    def shared_wait(self):
        me = lax.axis_index("sp_2")
        for s, i in self.services():
            for way in (0, 1):
                self.partner_copy(s, way, (i, 1 - i)[way], 1 - me).wait_recv()

    def drain(self):
        me = lax.axis_index("sp_2")
        for s, i in self.services():
            for c in self.sends(s, i):
                c.wait_send()
            if self.shared:
                for way in (0, 1):
                    self.partner_copy(s, way, (i, 1 - i)[way], me).wait_send()


def sems(n):
    return pltpu.SemaphoreType.DMA((n,))


LAYER_SCRATCH = dict(
    act=pltpu.VMEM((512, 512), BF16), acts=pltpu.VMEM((4, 128, 512), BF16), rows_s=sems(3), rows_r=sems(3),
    g=pltpu.VMEM((3, 8, 4, 2, 32, 1408), BF16), wo=pltpu.VMEM((4, 2, 2, 128, 2048), BF16), load=sems(4),
    stream=pltpu.VMEM((128, 2048), BF16), normed=pltpu.VMEM((4, 2, 64, 2048), BF16),
    pre=pltpu.VMEM((2, 528, 1408), BF16), hidden=pltpu.VMEM((128, 1408), BF16),
    part=pltpu.VMEM((3, 2, 128, 1024), BF16), own=pltpu.VMEM((2, 128, 1024), F32),
    far=pltpu.VMEM((2, 128, 1024), BF16), near=pltpu.VMEM((2, 2, 128, 1024), BF16),
    ax_s=sems(8), ax_r=sems(8), bz_s=sems(16), bz_r=sems(16), az_s=sems(16), az_r=sems(16), bx_s=sems(8), bx_r=sems(8),
    wy_s=sems(8), wy_r=sems(8), ny_s=sems(8), ny_r=sems(8), azp_s=sems(16), azp_r=sems(16), bxp_s=sems(8), bxp_r=sems(8),
    wyp_s=sems(8), wyp_r=sems(8), half_s=sems(2), half_r=sems(2), halo_s=sems(1), halo_r=sems(1), sum_s=sems(6), sum_r=sems(6),
)
SCRATCH = {**MIXER_SCRATCH, **EXCHANGE_SCRATCH, **LAYER_SCRATCH}
IN_VMEM = ("u", "damp", "ls", "rr", "ri", "inm", "outm", "skip", "residual", "gain", "taps")
IN_HBM = ("w_act", "w_lin", "w_dn", "w_out")


def layer_kernel(*refs):
    names = (*IN_VMEM, *IN_HBM, "out", *SCRATCH)
    r = Refs(**dict(zip(names, refs)))
    core, x, z, y = (lax.axis_index(a) for a in ("sp_2", "sp_1", "sp_0", "tp"))
    loads = [pltpu.make_async_copy(w, r.g.at[m, z, x, core], r.load.at[m]) for m, w in enumerate((r.w_act, r.w_lin, r.w_dn))]
    loads += [pltpu.make_async_copy(r.w_out.at[pl.ds((2 * c + k) * 128, 128), :], r.wo.at[y, c, k], r.load.at[3]) for c in (0, 1) for k in (0, 1)]
    for c in loads:
        c.start()
    r.got_z[...] = jnp.zeros_like(r.got_z)
    at = z * 8 + x * 2 + core

    def position(n):
        n = lax.rem(n, 64)
        return {"sp_0": n // 8, "sp_1": lax.rem(n, 8) // 2, "sp_2": lax.rem(n, 2)}

    following, previous = position(at + 1), position(at + 63)
    greet((("sp_2", 2), ("sp_1", 4), ("sp_0", 8), ("tp", 4)), [following, previous])
    for c in loads:
        c.wait()

    halves = (pl.ds(0, 768), pl.ds(768, 640))
    upper, lower = pl.ds(0, 16), pl.ds(16, 16)
    ax = Ring("sp_1", 4, lambda o, k: r.g.at[:, z, o, core, upper, halves[k]], r.ax_s, r.ax_r)
    bz = Ring("sp_0", 8, lambda o, k: r.g.at[:, o, x, core, lower, halves[k]], r.bz_s, r.bz_r)
    az = Ring("sp_0", 8, lambda o, k, c=core: r.g.at[:, o, pl.ds(2 * k, 2), c, upper, :], r.az_s, r.az_r, (r.azp_s, r.azp_r))
    bx = Ring("sp_1", 4, lambda o, k, c=core: r.g.at[:, pl.ds(4 * k, 4), o, c, lower, :], r.bx_s, r.bx_r, (r.bxp_s, r.bxp_r))
    wy = Ring("tp", 4, lambda o, k, c=core: r.wo.at[o, c, k], r.wy_s, r.wy_r, (r.wyp_s, r.wyp_r))
    ny = Ring("tp", 4, lambda o, k: r.normed.at[o, k], r.ny_s, r.ny_r)

    def half_copies(c):
        return [
            pltpu.make_async_remote_copy(
                src_ref=ref, dst_ref=ref, send_sem=r.half_s.at[n], recv_sem=r.half_r.at[n], device_id={"sp_2": 1 - core}, device_id_type=MESH
            )
            for n, ref in enumerate((r.g.at[:, z, :, c, upper, :], r.g.at[:, :, x, c, lower, :]))
        ]

    wy.begin()
    ax.begin()
    bz.begin()

    def at_point(n):
        if n == 0:
            ax.service(1, 0)
            ax.service(1, 1)
            bz.service(1, 0)
            bz.service(1, 1)
        elif n == 1:
            bz.service(2, 0)
            bz.service(2, 1)
            ax.service(2, 0)
        elif n == 2:
            bz.service(3, 0)
            bz.service(3, 1)
        elif n == 3:
            bz.service(4, 0)
        elif n == 4:
            wy.service(1, 0)
        elif n == 5:
            az.service(1, 0)
            wy.service(1, 1)

    def between():
        az.begin()
        bx.begin()
        for c in half_copies(core):
            c.start()

    mixer_phase(r, functools.partial(exchange, r, between), at_point)
    az.service(1, 1)
    bx.service(1, 0)
    wy.service(2, 0)
    for d in (2, 1, 3):
        to_rows(r, d).wait_recv()
    wy.shared_wait()

    def project(n, squares):
        cols = pl.ds(pl.multiple_of(n * 256, 256), 256)
        total = r.residual[:, cols].astype(F32)
        total += sum(jnp.dot(r.acts[q], r.wo[q, :, :, :, cols].reshape(512, 256), preferred_element_type=F32) for q in range(4))
        total = total.astype(BF16)
        r.stream[:, cols] = total
        total = total.astype(F32)
        return squares + total * total

    squares = lax.fori_loop(0, 8, project, jnp.zeros((128, 256), F32))
    scale = lax.rsqrt(jnp.sum(squares, axis=1, keepdims=True) / 2048 + 1e-06)

    def normalize(n, _):
        cols = pl.ds(pl.multiple_of(n * 256, 256), 256)
        v = (r.stream[:, cols].astype(F32) * scale * r.gain[:, cols]).astype(BF16)
        r.normed[y, :, :, cols] = v.reshape(2, 64, 256)
        return 0

    lax.fori_loop(0, 8, normalize, 0)
    ny.begin()
    az.service(2, 0)
    az.service(2, 1)
    ny.service(1, 0)
    bx.service(1, 1)
    az.service(3, 0)
    ny.service(1, 1)
    az.service(3, 1)
    bx.service(2, 0)
    ny.service(2, 0)
    az.service(4, 0)
    for c in half_copies(1 - core):
        c.wait_recv()
    bx.shared_wait()
    az.shared_wait()

    def up(h, cols, m):
        lhs = r.normed[pl.ds(2 * h, 2)].reshape(256, 2048)
        w = r.g[m, :, :, :, :, cols].reshape(2048, cols.size)
        out = jnp.dot(lhs, w, preferred_element_type=F32)
        r.pre[m, pl.ds(16 + 256 * h, 256), cols] = out.astype(BF16)

    def up_half(h):
        def tile(b, _):
            up(h, pl.ds(pl.multiple_of((b // 2) * 256, 256), 256), b % 2)
            return 0

        lax.fori_loop(0, 10, tile, 0)
        up(h, pl.ds(1280, 128), 0)
        up(h, pl.ds(1280, 128), 1)

    halo = pltpu.make_async_remote_copy(
        src_ref=r.pre.at[:, pl.ds(512, 16), :], dst_ref=r.pre.at[:, pl.ds(0, 16), :], send_sem=r.halo_s.at[0], recv_sem=r.halo_r.at[0],
        device_id=following, device_id_type=MESH,
    )
    up_half(1)
    halo.start()
    up_half(0)
    halo.wait_recv()
    starts = at == 0

    def convolved(b, m, cols):
        v = r.pre[m, pl.ds(pl.multiple_of(b * 128, 128), 144), cols].astype(F32)
        v = jnp.where(jnp.logical_and(jnp.logical_and(starts, b == 0), iota(v.shape, 0) < 16), 0.0, v)
        return sum(r.taps[k, pl.ds(m, 1), cols] * v[14 + k : 142 + k] for k in range(3))

    def hide(b):
        def tile(n, _):
            cols = pl.ds(pl.multiple_of(n * 128, 128), 128)
            a, l = convolved(b, 0, cols), convolved(b, 1, cols)
            r.hidden[:, cols] = (a / (1.0 + jnp.exp(-a)) * l).astype(BF16)
            return 0

        lax.fori_loop(0, 11, tile, 0)

    def down(put):
        def tile(n, _):
            w = r.g[2, pl.ds(n, 1)].reshape(256, 1408)
            put(n // 4, pl.ds(pl.multiple_of((n % 4) * 256, 256), 256), lax.dot_general(r.hidden[...], w, NT, preferred_element_type=F32))
            return 0

        lax.fori_loop(0, 8, tile, 0)

    def down_to(slot):
        def put(side, cols, v):
            r.part[slot, side, :, cols] = v.astype(BF16)

        down(put)

    def send_sum(n, src, dst, way):
        return pltpu.make_async_remote_copy(
            src_ref=src, dst_ref=dst, send_sem=r.sum_s.at[n], recv_sem=r.sum_r.at[n],
            device_id={"tp": lax.rem(y + (1, 3)[way], 4)}, device_id_type=MESH,
        )

    def sums():
        return [
            send_sum(0, r.part.at[0, 0], r.far.at[0], 0),
            send_sum(1, r.part.at[0, 1], r.far.at[1], 1),
            send_sum(2, r.part.at[1, 1], r.near.at[0, 1], 0),
            send_sum(3, r.part.at[2, 0], r.near.at[1, 0], 1),
            send_sum(4, r.part.at[1, 0], r.near.at[0, 0], 0),
            send_sum(5, r.part.at[2, 1], r.near.at[1, 1], 1),
        ]

    copies = sums()
    hide(lax.rem(y + 2, 4))
    down_to(0)
    copies[0].start()
    copies[1].start()
    hide(lax.rem(y + 1, 4))
    down_to(1)
    copies[2].start()
    hide(lax.rem(y + 3, 4))
    down_to(2)
    copies[3].start()
    copies[0].wait_recv()
    r.part[1, 0] = (r.part[1, 0].astype(F32) + r.far[0].astype(F32)).astype(BF16)
    copies[4].start()
    copies[1].wait_recv()
    r.part[2, 1] = (r.part[2, 1].astype(F32) + r.far[1].astype(F32)).astype(BF16)
    copies[5].start()
    hide(y)

    def keep(side, cols, v):
        r.own[side, :, cols] = v

    down(keep)
    for c in copies[2:]:
        c.wait_recv()
    for side in (0, 1):
        cols = pl.ds(side * 1024, 1024)
        total = r.own[side] + r.near[0, side].astype(F32) + r.near[1, side].astype(F32)
        r.out[:, cols] = (r.stream[:, cols].astype(F32) + total).astype(BF16)
    for ring in (ax, bz, az, bx, wy, ny):
        ring.drain()
    for c in (*half_copies(core), *copies, halo, *(to_rows(r, d) for d in (1, 2, 3))):
        c.wait_send()


def per_device(
    mixer_input, residual, log_step, rate_real, rate_imag, damping, in_map, out_map, skip, w_out, norm_gain, w_act, w_lin, conv_taps, w_down
):
    in_vmem = (
        mixer_input, damping.T, jnp.broadcast_to(log_step[:, None], rate_real.shape), rate_real, rate_imag,
        in_map.transpose(0, 1, 3, 2), out_map, skip[None], residual, norm_gain[None], conv_taps.transpose(1, 0, 2),
    )
    in_hbm = (w_act, w_lin, w_down.T, w_out)
    return pl.pallas_call(
        layer_kernel,
        out_shape=jax.ShapeDtypeStruct(residual.shape, BF16),
        in_specs=[pl.BlockSpec(memory_space=pltpu.VMEM)] * len(in_vmem) + [pl.BlockSpec(memory_space=pl.ANY)] * len(in_hbm),
        out_specs=pl.BlockSpec(memory_space=pltpu.VMEM),
        scratch_shapes=list(SCRATCH.values()),
        compiler_params=pltpu.CompilerParams(collective_id=0, has_side_effects=True, vmem_limit_bytes=60 * 2**20),
        name="layer",
    )(*in_vmem, *in_hbm)


def solution(mesh):
    split = Mesh(mesh.devices.reshape(8, 4, 2, mesh.shape["tp"]), ("sp_0", "sp_1", "sp_2", "tp"))
    in_specs = (
        P(SP, "tp"),
        P(SP_TP, None),
        P("tp"),
        P("tp", None),
        P("tp", None),
        P(SP, "tp"),
        P(None, "tp", None, None),
        P(None, "tp", None, None),
        P("tp"),
        P("tp", None),
        P(),
        P(SP, "tp"),
        P(SP, "tp"),
        P(None, None, "tp"),
        P("tp", SP),
    )
    out_specs = P(SP_TP, None)
    return jax.shard_map(
        per_device, mesh=split, in_specs=in_specs, out_specs=out_specs, check_vma=False
    )
```

```python
import functools

import jax
import jax.numpy as jnp
from jax import lax
from jax.experimental import pallas as pl
from jax.experimental.pallas import tpu as pltpu
from jax.sharding import Mesh
from jax.sharding import PartitionSpec as P

F32, BF16 = jnp.float32, jnp.bfloat16
NT = (((1,), (1,)), ((), ()))
TN = (((0,), (0,)), ((), ()))
Q, CH, PAIRS = 8, 64, 16
SP = ("sp_0", "sp_1", "sp_2")
SP_TP = ("sp_0", "sp_1", "sp_2", "tp")
MESH = pl.DeviceIdType.MESH

def iota(shape, dim):
    return lax.broadcasted_iota(jnp.int32, shape, dim)

def cmul(ar, ai, br, bi):
    return ar * br - ai * bi, ar * bi + ai * br

def split3(x):
    hi = x.astype(BF16)
    r = x - hi.astype(F32)
    mid = r.astype(BF16)
    lo = (r - mid.astype(F32)).astype(BF16)
    return hi, mid, lo

def block_swap(parts):
    parts = list(parts)
    block = iota(parts[0].shape, 1) // 16
    for b in (4, 2, 1):
        here = (block // b) % 2 == 0
        for n in range(8):
            if n & b == 0:
                low, high = parts[n], parts[n + b]
                parts[n] = jnp.where(here, low, pltpu.roll(high, 16 * b, axis=1))
                parts[n + b] = jnp.where(here, pltpu.roll(low, 128 - 16 * b, axis=1), high)
    return parts


def paired(even, odd):
    return jnp.concatenate([even, odd], axis=1)


def mixer_phase(r, greeted, comm, at_point):
    def rows(ref):
        return paired(ref[pl.ds(0, PAIRS, stride=2), :], ref[pl.ds(1, PAIRS, stride=2), :])

    rr, ri = rows(r.rr), rows(r.ri)
    step = jnp.exp(rows(r.ls))
    lr, th = rr * step, ri * step
    cos, sin = jnp.cos(th), jnp.sin(th)
    mag, inv = jnp.exp(lr), jnp.exp(-lr)
    ar, ai = mag * cos, mag * sin
    den = rr * rr + ri * ri
    r.fac[0] = ((ar - 1.0) * rr + ai * ri) / den
    r.fac[1] = (ai * rr - (ar - 1.0) * ri) / den
    one, zero = jnp.ones_like(ar), jnp.zeros_like(ar)
    pr, pi, nr, ni = one, zero, one, zero
    for s in range(Q):
        at = pl.ds(s, PAIRS, stride=Q)
        r.pw[0, at, :], r.pw[1, at, :] = nr, ni
        r.pw[2, at, :], r.pw[3, at, :] = pr, pi
        pr, pi = cmul(pr, pi, ar, ai)
        nr, ni = cmul(nr, ni, inv * cos, -inv * sin)
    d = r.damp[...]
    lane = iota(d.shape, 1) % Q
    for sh in (1, 2, 4):
        d = d + jnp.where(lane >= sh, pltpu.roll(d, sh, axis=1), 0.0)
    ex = (iota((96, 512), 0) % 32 == iota((96, 512), 1) // 16).astype(F32).astype(BF16)
    def spread_out(v):
        parts = jnp.concatenate([p.astype(F32) for p in split3(v)], axis=0).astype(BF16)
        return lax.dot_general(parts, ex, TN, preferred_element_type=F32)

    pick = (iota((CH, 512), 1) == Q * iota((CH, 512), 0) + Q - 1).astype(F32).astype(BF16)
    ends = sum(lax.dot_general(pick, p, NT, preferred_element_type=F32) for p in split3(d))
    ends = jnp.exp(ends)
    low = iota((CH, 128), 1) < 64
    for k in range(PAIRS):
        r.e7[pl.ds(k, CH, stride=PAIRS), :] = jnp.where(low, ends[:, 2 * k : 2 * k + 1], ends[:, 2 * k + 1 : 2 * k + 2])

    greeted()
    shrink = spread_out(jnp.exp(-d)) * r.u[...].astype(F32)
    for j in range(4):
        r.v[j] = shrink[:, j * 128 : j * 128 + 128]

    def spread(b, _):
        j, c = b // 2, b % 2
        parts = block_swap([r.v[j, pl.ds(c * 256 + n, 32, stride=8), :] for n in range(8)])
        for n in range(8):
            r.z[j * 8 + n, pl.ds(pl.multiple_of(c * 32, 32), 32), :] = parts[n]
        return 0

    lax.fori_loop(0, 8, spread, 0)

    low = iota((128, 128), 1) < 64

    def stacked(re, im):
        top = jnp.concatenate([jnp.where(low, re, 0.0), jnp.where(low, im, 0.0)], axis=1)
        bottom = jnp.concatenate([jnp.where(low, 0.0, re), jnp.where(low, 0.0, im)], axis=1)
        return jnp.concatenate([top, bottom], axis=0).astype(BF16)

    def outer(which, k, br, bi):
        at = pl.ds(pl.multiple_of(k * Q, Q), Q)
        wr, wi = r.pw[which, at, :][:, None, :], r.pw[which + 1, at, :][:, None, :]
        br, bi = br[None], bi[None]
        re, im = cmul(wr, wi, br, bi)
        return re.reshape(128, 128), im.reshape(128, 128)

    def inputs_of(k):
        return jnp.concatenate([r.z[2 * k], r.z[2 * k + 1]], axis=1).astype(BF16)

    def states_in(k, _):
        br, bi = paired(r.inm[0, 2 * k], r.inm[0, 2 * k + 1]), paired(r.inm[1, 2 * k], r.inm[1, 2 * k + 1])
        br, bi = cmul(r.fac[0, pl.ds(k, 1), :], r.fac[1, pl.ds(k, 1), :], br, bi)
        p = stacked(*outer(0, k, br, bi))
        r.pb[k] = p
        s = jnp.dot(inputs_of(k), p, preferred_element_type=F32)
        at = pl.ds(k, CH, stride=PAIRS)
        r.sr[at, :] = s[:, :128]
        r.si[at, :] = s[:, 128:]
        return 0

    lax.fori_loop(0, PAIRS, states_in, 0, unroll=2)

    a2r, a2i = cmul(ar, ai, ar, ai)
    a4r, a4i = cmul(a2r, a2i, a2r, a2i)
    a8r, a8i = cmul(a4r, a4i, a4r, a4i)

    def advance(c, carry, keep):
        vr, vi, e_all = carry
        at = pl.ds(pl.multiple_of(c * PAIRS, PAIRS), PAIRS)
        e = r.e7[at, :]
        tr, ti = (vr + r.sr[at, :]) * e, (vi + r.si[at, :]) * e
        if keep:
            r.sr[at, :], r.si[at, :] = vr, vi
        vr, vi = cmul(a8r, a8i, tr, ti)
        return vr, vi, e_all * e

    vr, vi, e_all = lax.fori_loop(0, CH, functools.partial(advance, keep=False), (zero, zero, one), unroll=8)

    at_point(0)
    causal = (iota((256, 256), 0) // 16) % Q <= (iota((256, 256), 1) // 16) % Q

    def inside(k, _):
        cr, ci = paired(r.outm[0, 2 * k], r.outm[0, 2 * k + 1]), paired(r.outm[1, 2 * k], r.outm[1, 2 * k + 1])
        qr, qi = outer(2, k, cr, ci)
        q = stacked(qr, -qi)
        r.qb[k] = q
        m = lax.dot_general(r.pb[k], q, NT, preferred_element_type=F32)
        m = jnp.where(causal, m, 0.0).astype(BF16)
        out = jnp.dot(inputs_of(k), m, preferred_element_type=F32)
        r.y[2 * k] = out[:, :128]
        r.y[2 * k + 1] = out[:, 128:]
        return 0

    def inside_part(n):
        cuts = (0, 6, 12, 16)
        lax.fori_loop(cuts[n], cuts[n + 1], inside, 0, unroll=2)

    vr, vi = comm(ar, ai, vr, vi, e_all, inside_part)
    r.ex[...] = spread_out(jnp.exp(d))
    lax.fori_loop(0, CH, functools.partial(advance, keep=True), (vr, vi, one), unroll=8)

    def outputs(k, _):
        at = pl.ds(k, CH, stride=PAIRS)
        v = jnp.concatenate([r.sr[at, :], r.si[at, :]], axis=1).astype(BF16)
        out = lax.dot_general(v, r.qb[k], NT, preferred_element_type=F32)
        r.y[2 * k] += out[:, :128]
        r.y[2 * k + 1] += out[:, 128:]
        return 0

    lax.fori_loop(0, PAIRS, outputs, 0, unroll=2)
    at_point(1)


def finish_rows(r, q):
    rows = pl.ds(pl.multiple_of(q * 128, 128), 128)

    def turn(j, _):
        parts = block_swap([r.y[j * 8 + n, pl.ds(pl.multiple_of(q * 16, 16), 16), :] for n in range(8)])
        for n in range(8):
            r.v[j, pl.ds(q * 128 + n, 16, stride=8), :] = parts[n]
        return 0

    def close(j, _):
        lanes = pl.ds(pl.multiple_of(j * 128, 128), 128)
        mixed = r.v[j, rows, :] * r.ex[rows, lanes] + r.skip[:, lanes] * r.u[rows, lanes].astype(F32)
        r.act[rows, lanes] = jax.nn.gelu(mixed).astype(BF16)
        return 0

    lax.fori_loop(0, 4, turn, 0, unroll=2)
    lax.fori_loop(0, 4, close, 0, unroll=2)


def fold(acc, vr, vi, e, wr, wi, use):
    er, ei = cmul(wr * e, wi * e, acc[0], acc[1])
    return jnp.where(use, er + vr, acc[0]), jnp.where(use, ei + vi, acc[1]), jnp.where(use, acc[2] * e, acc[2])


def squared(w, times):
    for _ in range(times):
        w = cmul(*w, *w)
    return w


class Refs:
    def __init__(self, **named):
        self.__dict__.update(named)


MIXER_SCRATCH = dict(
    fac=pltpu.VMEM((2, PAIRS, 128), F32), pw=pltpu.VMEM((4, PAIRS * Q, 128), F32), ex=pltpu.VMEM((512, 512), F32), v=pltpu.VMEM((4, 512, 128), F32),
    e7=pltpu.VMEM((CH * PAIRS, 128), F32), z=pltpu.VMEM((32, CH, 128), F32), y=pltpu.VMEM((32, CH, 128), F32),
    pb=pltpu.VMEM((PAIRS, 256, 256), BF16), qb=pltpu.VMEM((PAIRS, 256, 256), BF16),
    sr=pltpu.VMEM((CH * PAIRS, 128), F32), si=pltpu.VMEM((CH * PAIRS, 128), F32),
)


EXCHANGE_SCRATCH = dict(
    mine=pltpu.VMEM((3, 3, PAIRS, 128), F32), got_c=pltpu.VMEM((1, 3, PAIRS, 128), F32), got_x=pltpu.VMEM((3, 3, PAIRS, 128), F32),
    got_z=pltpu.VMEM((7, 3, PAIRS, 128), F32), ssem=pltpu.SemaphoreType.DMA((11,)), rsem=pltpu.SemaphoreType.DMA((11,)),
)


def greet(groups, others):
    barrier = pltpu.get_barrier_semaphore()
    peers = [{axis: lax.rem(lax.axis_index(axis) + d, count)} for axis, count in groups for d in range(1, count)] + others
    for peer in peers:
        pl.semaphore_signal(barrier, inc=1, device_id=peer, device_id_type=MESH)
    return lambda: pl.semaphore_wait(barrier, len(peers))


def exchange(r, after_x, after_z, ar, ai, vr, vi, e, part):
    core, x, z = lax.axis_index("sp_2"), lax.axis_index("sp_1"), lax.axis_index("sp_0")

    def copies(level, axis, me, count, got, first):
        return [
            pltpu.make_async_remote_copy(
                src_ref=r.mine.at[level], dst_ref=got.at[d - 1], send_sem=r.ssem.at[first + d - 1], recv_sem=r.rsem.at[first + d - 1],
                device_id={axis: lax.rem(me + d, count)}, device_id_type=MESH,
            )
            for d in range(1, count)
        ]

    def put(level, parts):
        for n, v in enumerate(parts):
            r.mine[level, n] = v

    def of(got, slot):
        return got[slot, 0], got[slot, 1], got[slot, 2]

    nothing = (jnp.zeros_like(vr), jnp.zeros_like(vr), jnp.ones_like(vr))
    w1 = squared((ar, ai), 9)
    w2 = squared(w1, 1)
    w8 = squared(w2, 2)
    own = (vr, vi, e)
    put(0, own)
    for c in copies(0, "sp_2", core, 2, r.got_c, 0):
        c.start()
    part(0)
    for c in copies(0, "sp_2", core, 2, r.got_c, 0):
        c.wait()
    other = of(r.got_c, 0)
    early = [jnp.where(core == 0, a, b) for a, b in zip(own, other)]
    late = [jnp.where(core == 0, b, a) for a, b in zip(own, other)]
    chip = fold(early, *late, *w1, True)
    put(1, chip)
    for c in copies(1, "sp_1", x, 4, r.got_x, 1):
        c.start()
    after_x()
    part(1)
    for c in copies(1, "sp_1", x, 4, r.got_x, 1):
        c.wait()
    total = nothing
    for d in (3, 2, 1):
        total = fold(total, *of(r.got_x, d - 1), *w2, d <= x)
    total = fold(total, *chip, *w2, True)
    for d in (3, 2, 1):
        total = fold(total, *of(r.got_x, d - 1), *w2, d > x)
    put(2, total)
    sends = copies(2, "sp_0", z, 8, r.got_z, 4)
    for d in range(1, 8):
        pl.when(z + d < 8)(sends[d - 1].start)
    after_z()
    part(2)
    for d in range(1, 8):
        pl.when(z + d < 8)(sends[d - 1].wait_send)
        pl.when(z >= d)(sends[d - 1].wait_recv)
    enter = nothing
    for d in range(7, 0, -1):
        enter = fold(enter, *of(r.got_z, d - 1), *w8, d <= z)
    for d in (3, 2, 1):
        enter = fold(enter, *of(r.got_x, d - 1), *w2, d <= x)
    enter = fold(enter, *other, *w1, core == 1)
    return enter[0], enter[1]

class Ring:
    def __init__(self, axis, count, many, chunk, ssem, rsem, swap=False, shared=None):
        self.axis, self.count, self.many, self.chunk, self.ssem, self.rsem = axis, count, many, chunk, ssem, rsem
        self.swap, self.shared = swap, shared
        self.me, self.half = lax.axis_index(axis), count // 2

    def place(self, steps):
        return lax.rem(self.me + steps + self.count, self.count)

    def moves(self, step, i):
        for way in (0, 1):
            j = i ^ way if self.swap else i
            if step < self.half or (step == self.half and j % 2 == way):
                yield way, j

    def copy(self, step, way, j, owner):
        n = ((step - 1) * 2 + way) * self.many + j
        ref = self.chunk(self.place(owner), j)
        return pltpu.make_async_remote_copy(
            src_ref=ref, dst_ref=ref, send_sem=self.ssem.at[n], recv_sem=self.rsem.at[n],
            device_id={self.axis: self.place(1 - 2 * way)}, device_id_type=MESH,
        )

    def partner_copy(self, step, way, j, core):
        n = ((step - 1) * 2 + way) * self.many + j
        ref = self.chunk(self.place((2 * way - 1) * step), j, core)
        return pltpu.make_async_remote_copy(
            src_ref=ref, dst_ref=ref, send_sem=self.shared[0].at[n], recv_sem=self.shared[1].at[n],
            device_id={"sp_2": 1 - lax.axis_index("sp_2")}, device_id_type=MESH,
        )

    def start(self, i):
        for way, j in self.moves(1, i):
            self.copy(1, way, j, 0).start()

    def service(self, step, i):
        onward = list(self.moves(step + 1, i))
        for way, j in self.moves(step, i):
            self.copy(step, way, j, (2 * way - 1) * step).wait_recv()
            if (way, j) in onward:
                self.copy(step + 1, way, j, (2 * way - 1) * step).start()
            if self.shared:
                self.partner_copy(step, way, j, lax.axis_index("sp_2")).start()

    def all_moves(self):
        return [(s, way, j) for s in range(1, self.half + 1) for i in range(self.many) for way, j in self.moves(s, i)]

    def shared_wait(self):
        for s, way, j in self.all_moves():
            self.partner_copy(s, way, j, 1 - lax.axis_index("sp_2")).wait_recv()

    def drain(self):
        for s, way, j in self.all_moves():
            self.copy(s, way, j, (2 * way - 1) * (s - 1)).wait_send()
            if self.shared:
                self.partner_copy(s, way, j, lax.axis_index("sp_2")).wait_send()


class RowSum:
    def __init__(self, r, n, prepare, product):
        self.part, self.far, self.near, self.own = r.part.at[n], r.far.at[n], r.near.at[n], r.own
        self.ssem, self.rsem, self.y = r.sum_s.at[n], r.sum_r.at[n], lax.axis_index("tp")
        self.prepare, self.product = prepare, product
        part, far, near = self.part, self.far, self.near
        self.copies = [
            self.copy(0, part.at[0, 0], far.at[0], 1), self.copy(1, part.at[0, 1], far.at[1], 3),
            self.copy(2, part.at[1, 1], near.at[0, 1], 1), self.copy(3, part.at[2, 0], near.at[1, 0], 3),
            self.copy(4, part.at[1, 0], near.at[0, 0], 1), self.copy(5, part.at[2, 1], near.at[1, 1], 3),
        ]

    def copy(self, n, src, dst, d):
        return pltpu.make_async_remote_copy(
            src_ref=src, dst_ref=dst, send_sem=self.ssem.at[n], recv_sem=self.rsem.at[n],
            device_id={"tp": lax.rem(self.y + d, 4)}, device_id_type=MESH,
        )

    def others(self, busy):
        for slot, d in enumerate((2, 1, 3)):
            block = lax.rem(self.y + d, 4)

            def put(side, cols, v):
                self.part[slot, side, :, cols] = v.astype(BF16)

            self.prepare(block)
            self.product(block, put)
            for c in ((0, 1), (2,), (3,))[slot]:
                self.copies[c].start()
            busy(slot)

    def mine(self):
        def put(side, cols, v):
            self.own[side, :, cols] = v

        self.prepare(self.y)
        self.product(self.y, put)

    def pass_on(self):
        for n, slot, side in ((0, 1, 0), (1, 2, 1)):
            self.copies[n].wait_recv()
            self.part[slot, side] = (self.part[slot, side].astype(F32) + self.far[n].astype(F32)).astype(BF16)
            self.copies[4 + n].start()

    def arrived(self):
        for c in self.copies[2:]:
            c.wait_recv()

    def total(self, side, cols):
        return self.own[side, :, cols] + self.near[0, side, :, cols].astype(F32) + self.near[1, side, :, cols].astype(F32)

    def drain(self):
        for c in self.copies:
            c.wait_send()


def sems(n):
    return pltpu.SemaphoreType.DMA((n,))


LAYER_SCRATCH = dict(
    act=pltpu.VMEM((512, 512), BF16), g=pltpu.VMEM((3, 8, 4, 2, 32, 1408), BF16), load=sems(3),
    stream=pltpu.VMEM((128, 2048), BF16), normed=pltpu.VMEM((33, 16, 2048), BF16),
    pre=pltpu.VMEM((2, 528, 1408), BF16), hidden=pltpu.VMEM((128, 1408), BF16),
    part=pltpu.VMEM((2, 3, 2, 128, 1024), BF16), own=pltpu.VMEM((2, 128, 1024), F32),
    far=pltpu.VMEM((2, 2, 128, 1024), BF16), near=pltpu.VMEM((2, 2, 2, 128, 1024), BF16),
    ax_s=sems(8), ax_r=sems(8), bz_s=sems(16), bz_r=sems(16), az_s=sems(32), az_r=sems(32), bx_s=sems(32), bx_r=sems(32),
    ny_s=sems(8), ny_r=sems(8), azp_s=sems(32), azp_r=sems(32), bxp_s=sems(32), bxp_r=sems(32),
    half_s=sems(2), half_r=sems(2), halo_s=sems(4), halo_r=sems(1),
    sum_s=pltpu.SemaphoreType.DMA((2, 6)), sum_r=pltpu.SemaphoreType.DMA((2, 6)),
)
SCRATCH = {**MIXER_SCRATCH, **EXCHANGE_SCRATCH, **LAYER_SCRATCH}
IN_VMEM = ("u", "damp", "ls", "rr", "ri", "inm", "outm", "skip", "residual", "gain", "taps", "w_out")
IN_HBM = ("w_act", "w_lin", "w_dn")


def layer_kernel(*refs):
    names = (*IN_VMEM, *IN_HBM, "out", *SCRATCH)
    r = Refs(**dict(zip(names, refs)))
    core, x, z, y = (lax.axis_index(a) for a in ("sp_2", "sp_1", "sp_0", "tp"))
    loads = [pltpu.make_async_copy(w, r.g.at[m, z, x, core], r.load.at[m]) for m, w in enumerate((r.w_act, r.w_lin, r.w_dn))]
    for c in loads:
        c.start()
    r.got_z[...] = jnp.zeros_like(r.got_z)
    at = z * 8 + x * 2 + core

    @pl.when(at == 0)
    def _():
        r.normed[0] = jnp.zeros((16, 2048), BF16)

    def position(n, tp):
        n = lax.rem(n, 64)
        return {"sp_0": n // 8, "sp_1": lax.rem(n, 8) // 2, "sp_2": lax.rem(n, 2), "tp": tp}

    beside = [position(at + n, q) for n in (1, 63) for q in range(4)]
    wait_for_all = greet((("sp_2", 2), ("sp_1", 4), ("sp_0", 8), ("tp", 4)), beside)

    a_cols, b_cols = pl.ds(0, 640), pl.ds(640, 768)
    a_half, b_half = (pl.ds(0, 384), pl.ds(384, 256)), (pl.ds(640, 384), pl.ds(1024, 384))
    beside_x = [lax.rem(x + n, 4) for n in (0, 1, 3, 2)]
    beside_z = [lax.rem(z + n, 8) for n in (0, 1, 7, 2, 6, 3, 5, 4)]
    ax = Ring("sp_1", 4, 2, lambda o, j: r.g.at[:, z, o, core, :, a_half[j]], r.ax_s, r.ax_r, True)
    bz = Ring("sp_0", 8, 2, lambda o, j: r.g.at[:, o, x, core, :, b_half[j]], r.bz_s, r.bz_r, True)
    az = Ring("sp_0", 8, 4, lambda o, j, c=core: r.g.at[:, o, beside_x[j], c, :, a_cols], r.az_s, r.az_r, False, (r.azp_s, r.azp_r))
    bx = Ring("sp_1", 4, 8, lambda o, j, c=core: r.g.at[:, beside_z[j], o, c, :, b_cols], r.bx_s, r.bx_r, False, (r.bxp_s, r.bxp_r))
    ny = Ring("tp", 4, 2, lambda o, j: r.normed.at[pl.ds(1 + o * 8 + j * 4, 4)], r.ny_s, r.ny_r, True)

    def half_copies(c):
        return [
            pltpu.make_async_remote_copy(
                src_ref=ref, dst_ref=ref, send_sem=r.half_s.at[n], recv_sem=r.half_r.at[n], device_id={"sp_2": 1 - core}, device_id_type=MESH
            )
            for n, ref in enumerate((r.g.at[:, z, :, c, :, a_cols], r.g.at[:, :, x, c, :, b_cols]))
        ]

    def serve(*steps):
        for ring, step, i in steps:
            ring.service(step, i)

    def greeted():
        for c in loads:
            c.wait()
        wait_for_all()
        for i in (0, 1):
            ax.start(i)
            bz.start(i)
        bx.start(0)
        az.start(0)

    def at_point(n):
        if n == 0:
            serve((ax, 1, 0), (ax, 1, 1), (bz, 1, 0), (bz, 1, 1))
        else:
            serve((az, 1, 1))

    def after_x():
        az.start(1)
        bx.start(1)
        bx.start(2)

    def after_z():
        az.start(2)
        serve((bz, 2, 0), (bz, 2, 1), (ax, 2, 0))
        az.start(3)
        serve((az, 1, 0))
        bx.start(3)
        bx.start(4)
        serve((bx, 1, 0))

    mixer_phase(r, greeted, functools.partial(exchange, r, after_x, after_z), at_point)

    def project(b, put):
        rows = pl.ds(pl.multiple_of(b * 128, 128), 128)

        def tile(n, _):
            cols = pl.ds(pl.multiple_of(n * 512, 512), 512)
            v = jnp.dot(r.act[rows, :], r.w_out[:, cols], preferred_element_type=F32)
            put(n // 2, pl.ds(pl.multiple_of((n % 2) * 512, 512), 512), v)
            return 0

        lax.fori_loop(0, 4, tile, 0)

    def while_projecting(slot):
        if slot == 2:
            serve((az, 1, 2), (bx, 1, 1), (bx, 1, 2))

    first = RowSum(r, 0, functools.partial(finish_rows, r), project)
    first.others(while_projecting)
    first.mine()
    serve((bz, 3, 0), (bz, 3, 1))
    bx.start(5)
    bx.start(6)
    first.pass_on()
    serve((az, 1, 3), (bx, 1, 3), (az, 2, 0), (bx, 1, 4), (bz, 4, 0))
    bx.start(7)
    for c in half_copies(core):
        c.start()
    serve((az, 2, 1), (bx, 1, 5), (az, 2, 2))
    first.arrived()

    def add_up(n, squares):
        cols = pl.ds(pl.multiple_of(n * 256, 256), 256)
        total = r.residual[:, cols].astype(F32) + first.total(n // 4, pl.ds(pl.multiple_of((n % 4) * 256, 256), 256))
        total = total.astype(BF16)
        r.stream[:, cols] = total
        total = total.astype(F32)
        return squares + total * total

    squares = lax.fori_loop(0, 8, add_up, jnp.zeros((128, 256), F32))
    scale = lax.rsqrt(jnp.sum(squares, axis=1, keepdims=True) / 2048 + 1e-06)

    def normalize(n, _):
        cols = pl.ds(pl.multiple_of(n * 256, 256), 256)
        v = (r.stream[:, cols].astype(F32) * scale * r.gain[:, cols]).astype(BF16)
        r.normed[pl.ds(1 + 8 * y, 8), :, cols] = v.reshape(8, 16, 256)
        return 0

    lax.fori_loop(0, 8, normalize, 0)
    ny.start(0)
    ny.start(1)
    halos = [
        pltpu.make_async_remote_copy(
            src_ref=r.normed.at[32], dst_ref=r.normed.at[0], send_sem=r.halo_s.at[q], recv_sem=r.halo_r.at[0],
            device_id=position(at + 1, q), device_id_type=MESH,
        )
        for q in range(4)
    ]
    ends = jnp.logical_and(y == 3, at < 63)

    @pl.when(ends)
    def _():
        for c in halos:
            c.start()

    serve((az, 2, 3), (bx, 1, 6), (az, 3, 0), (bx, 1, 7), (az, 3, 1), (az, 3, 2), (ny, 1, 0), (az, 3, 3))
    serve(*((bx, 2, j) for j in range(8)))
    serve((az, 4, 0), (az, 4, 1), (ny, 1, 1), (az, 4, 2), (az, 4, 3))
    for c in half_copies(1 - core):
        c.wait_recv()
    bx.shared_wait()
    az.shared_wait()
    pl.when(at > 0)(halos[0].wait_recv)
    serve((ny, 2, 0))

    def up(w, m, cols):
        out = jnp.dot(r.normed[...].reshape(528, 2048), w, preferred_element_type=F32)
        r.pre[m, :, cols] = out.astype(BF16)

    def up_tile(b, _):
        cols = pl.ds(pl.multiple_of((b // 2) * 256, 256), 256)
        up(r.g[b % 2, :, :, :, :, cols].reshape(2048, 256), b % 2, cols)
        return 0

    lax.fori_loop(0, 10, up_tile, 0)
    tail = pl.ds(1280, 128)
    w = jnp.concatenate([r.g[m, :, :, :, :, tail].reshape(2048, 128) for m in (0, 1)], axis=1)
    out = jnp.dot(r.normed[...].reshape(528, 2048), w, preferred_element_type=F32).astype(BF16)
    r.pre[0, :, tail], r.pre[1, :, tail] = out[:, :128], out[:, 128:]

    def convolved(b, m, cols):
        v = r.pre[m, pl.ds(pl.multiple_of(b * 128, 128), 144), cols].astype(F32)
        return sum(r.taps[k, pl.ds(m, 1), cols] * v[14 + k : 142 + k] for k in range(3))

    def hide(b):
        def tile(n, _):
            cols = pl.ds(pl.multiple_of(n * 128, 128), 128)
            a, l = convolved(b, 0, cols), convolved(b, 1, cols)
            r.hidden[:, cols] = (a / (1.0 + jnp.exp(-a)) * l).astype(BF16)
            return 0

        lax.fori_loop(0, 11, tile, 0)

    def down(b, put):
        def tile(n, _):
            w = r.g[2, pl.ds(n, 1)].reshape(256, 1408)
            put(n // 4, pl.ds(pl.multiple_of((n % 4) * 256, 256), 256), lax.dot_general(r.hidden[...], w, NT, preferred_element_type=F32))
            return 0

        lax.fori_loop(0, 8, tile, 0)

    second = RowSum(r, 1, hide, down)
    second.others(lambda slot: None)
    second.pass_on()
    second.mine()
    second.arrived()

    def close(n, _):
        cols = pl.ds(pl.multiple_of(n * 256, 256), 256)
        total = second.total(n // 4, pl.ds(pl.multiple_of((n % 4) * 256, 256), 256))
        r.out[:, cols] = (r.stream[:, cols].astype(F32) + total).astype(BF16)
        return 0

    lax.fori_loop(0, 8, close, 0, unroll=2)
    for ring in (ax, bz, az, bx, ny):
        ring.drain()
    for c in half_copies(core):
        c.wait_send()
    first.drain()
    second.drain()

    @pl.when(ends)
    def _():
        for c in halos:
            c.wait_send()


def per_device(
    mixer_input, residual, log_step, rate_real, rate_imag, damping, in_map, out_map, skip, w_out, norm_gain, w_act, w_lin, conv_taps, w_down
):
    in_vmem = (
        mixer_input, damping.T, jnp.broadcast_to(log_step[:, None], rate_real.shape), rate_real, rate_imag,
        in_map.transpose(0, 1, 3, 2), out_map, skip[None], residual, norm_gain[None], conv_taps.transpose(1, 0, 2), w_out,
    )
    in_hbm = (w_act, w_lin, w_down.T)
    return pl.pallas_call(
        layer_kernel,
        out_shape=jax.ShapeDtypeStruct(residual.shape, BF16),
        in_specs=[pl.BlockSpec(memory_space=pltpu.VMEM)] * len(in_vmem) + [pl.BlockSpec(memory_space=pl.ANY)] * len(in_hbm),
        out_specs=pl.BlockSpec(memory_space=pltpu.VMEM),
        scratch_shapes=list(SCRATCH.values()),
        compiler_params=pltpu.CompilerParams(collective_id=0, has_side_effects=True, vmem_limit_bytes=60 * 2**20),
        name="layer",
    )(*in_vmem, *in_hbm)


def solution(mesh):
    split = Mesh(mesh.devices.reshape(8, 4, 2, mesh.shape["tp"]), ("sp_0", "sp_1", "sp_2", "tp"))
    in_specs = (
        P(SP, "tp"),
        P(SP_TP, None),
        P("tp"),
        P("tp", None),
        P("tp", None),
        P(SP, "tp"),
        P(None, "tp", None, None),
        P(None, "tp", None, None),
        P("tp"),
        P("tp", None),
        P(),
        P(SP, "tp"),
        P(SP, "tp"),
        P(None, None, "tp"),
        P("tp", SP),
    )
    out_specs = P(SP_TP, None)
    return jax.shard_map(
        per_device, mesh=split, in_specs=in_specs, out_specs=out_specs, check_vma=False
    )
```

```python
import functools

import jax
import jax.numpy as jnp
from jax import lax
from jax.experimental import pallas as pl
from jax.experimental.pallas import tpu as pltpu
from jax.sharding import Mesh
from jax.sharding import PartitionSpec as P

F32, BF16 = jnp.float32, jnp.bfloat16
NT = (((1,), (1,)), ((), ()))
TN = (((0,), (0,)), ((), ()))
Q, CH, PAIRS = 8, 64, 16
SP = ("sp_0", "sp_1", "sp_2")
SP_TP = ("sp_0", "sp_1", "sp_2", "tp")
MESH = pl.DeviceIdType.MESH

def iota(shape, dim):
    return lax.broadcasted_iota(jnp.int32, shape, dim)

def cmul(ar, ai, br, bi):
    return ar * br - ai * bi, ar * bi + ai * br

def split3(x):
    hi = x.astype(BF16)
    r = x - hi.astype(F32)
    mid = r.astype(BF16)
    lo = (r - mid.astype(F32)).astype(BF16)
    return hi, mid, lo

def block_swap(parts):
    parts = list(parts)
    block = iota(parts[0].shape, 1) // 16
    for b in (4, 2, 1):
        here = (block // b) % 2 == 0
        for n in range(8):
            if n & b == 0:
                low, high = parts[n], parts[n + b]
                parts[n] = jnp.where(here, low, pltpu.roll(high, 16 * b, axis=1))
                parts[n + b] = jnp.where(here, pltpu.roll(low, 128 - 16 * b, axis=1), high)
    return parts


def paired(even, odd):
    return jnp.concatenate([even, odd], axis=1)


def mixer_phase(r, greeted, comm):
    def rows(ref):
        return paired(ref[pl.ds(0, PAIRS, stride=2), :], ref[pl.ds(1, PAIRS, stride=2), :])

    square = iota((32, 32), 0) == iota((32, 32), 1)
    r.steps[...] = jnp.broadcast_to(jnp.sum(jnp.where(square, r.ls[...], 0.0), axis=1, keepdims=True), (32, 64))
    rr, ri = rows(r.rr), rows(r.ri)
    step = jnp.exp(rows(r.steps))
    lr, th = rr * step, ri * step
    cos, sin = jnp.cos(th), jnp.sin(th)
    mag, inv = jnp.exp(lr), jnp.exp(-lr)
    ar, ai = mag * cos, mag * sin
    den = rr * rr + ri * ri
    r.fac[0] = ((ar - 1.0) * rr + ai * ri) / den
    r.fac[1] = (ai * rr - (ar - 1.0) * ri) / den
    one, zero = jnp.ones_like(ar), jnp.zeros_like(ar)
    pr, pi, nr, ni = one, zero, one, zero
    for s in range(Q):
        at = pl.ds(s, PAIRS, stride=Q)
        r.pw[0, at, :], r.pw[1, at, :] = nr, ni
        r.pw[2, at, :], r.pw[3, at, :] = pr, pi
        pr, pi = cmul(pr, pi, ar, ai)
        nr, ni = cmul(nr, ni, inv * cos, -inv * sin)
    d = r.damp[...]
    lane = iota(d.shape, 1) % Q
    for sh in (1, 2, 4):
        d = d + jnp.where(lane >= sh, pltpu.roll(d, sh, axis=1), 0.0)
    ex = (iota((96, 512), 0) % 32 == iota((96, 512), 1) // 16).astype(F32).astype(BF16)
    def spread_out(v):
        parts = jnp.concatenate([p.astype(F32) for p in split3(v)], axis=0).astype(BF16)
        return lax.dot_general(parts, ex, TN, preferred_element_type=F32)

    pick = (iota((CH, 512), 1) == Q * iota((CH, 512), 0) + Q - 1).astype(F32).astype(BF16)
    ends = sum(lax.dot_general(pick, p, NT, preferred_element_type=F32) for p in split3(d))
    ends = jnp.exp(ends)
    low = iota((CH, 128), 1) < 64
    for k in range(PAIRS):
        r.e7[pl.ds(k, CH, stride=PAIRS), :] = jnp.where(low, ends[:, 2 * k : 2 * k + 1], ends[:, 2 * k + 1 : 2 * k + 2])

    r.ex[...] = spread_out(jnp.exp(d))
    shrink = spread_out(jnp.exp(-d)) * r.u[...].astype(F32)
    for j in range(4):
        r.v[j] = shrink[:, j * 128 : j * 128 + 128]

    def spread(b, _):
        j, c = b // 2, b % 2
        parts = block_swap([r.v[j, pl.ds(c * 256 + n, 32, stride=8), :] for n in range(8)])
        for n in range(8):
            r.z[j * 8 + n, pl.ds(pl.multiple_of(c * 32, 32), 32), :] = parts[n]
        return 0

    lax.fori_loop(0, 8, spread, 0)
    greeted()

    low = iota((128, 128), 1) < 64

    def stacked(re, im):
        top = jnp.concatenate([jnp.where(low, re, 0.0), jnp.where(low, im, 0.0)], axis=1)
        bottom = jnp.concatenate([jnp.where(low, 0.0, re), jnp.where(low, 0.0, im)], axis=1)
        return jnp.concatenate([top, bottom], axis=0).astype(BF16)

    def outer(which, k, br, bi):
        at = pl.ds(pl.multiple_of(k * Q, Q), Q)
        wr, wi = r.pw[which, at, :][:, None, :], r.pw[which + 1, at, :][:, None, :]
        br, bi = br[None], bi[None]
        re, im = cmul(wr, wi, br, bi)
        return re.reshape(128, 128), im.reshape(128, 128)

    def inputs_of(k):
        return jnp.concatenate([r.z[2 * k], r.z[2 * k + 1]], axis=1).astype(BF16)

    def states_in(k, _):
        br, bi = paired(r.inm[0, 2 * k], r.inm[0, 2 * k + 1]), paired(r.inm[1, 2 * k], r.inm[1, 2 * k + 1])
        br, bi = cmul(r.fac[0, pl.ds(k, 1), :], r.fac[1, pl.ds(k, 1), :], br, bi)
        p = stacked(*outer(0, k, br, bi))
        r.pb[k] = p
        s = jnp.dot(inputs_of(k), p, preferred_element_type=F32)
        at = pl.ds(k, CH, stride=PAIRS)
        r.sr[at, :] = s[:, :128]
        r.si[at, :] = s[:, 128:]
        return 0

    lax.fori_loop(0, PAIRS, states_in, 0, unroll=2)

    a2r, a2i = cmul(ar, ai, ar, ai)
    a4r, a4i = cmul(a2r, a2i, a2r, a2i)
    a8r, a8i = cmul(a4r, a4i, a4r, a4i)

    def advance(c, carry, keep):
        vr, vi, e_all = carry
        at = pl.ds(pl.multiple_of(c * PAIRS, PAIRS), PAIRS)
        e = r.e7[at, :]
        tr, ti = (vr + r.sr[at, :]) * e, (vi + r.si[at, :]) * e
        if keep:
            r.sr[at, :], r.si[at, :] = vr, vi
        vr, vi = cmul(a8r, a8i, tr, ti)
        return vr, vi, e_all * e

    vr, vi, e_all = lax.fori_loop(0, CH, functools.partial(advance, keep=False), (zero, zero, one), unroll=8)

    causal = (iota((256, 256), 0) // 16) % Q <= (iota((256, 256), 1) // 16) % Q

    def inside(k, _):
        cr, ci = paired(r.outm[0, 2 * k], r.outm[0, 2 * k + 1]), paired(r.outm[1, 2 * k], r.outm[1, 2 * k + 1])
        qr, qi = outer(2, k, cr, ci)
        q = stacked(qr, -qi)
        r.qb[k] = q
        m = lax.dot_general(r.pb[k], q, NT, preferred_element_type=F32)
        m = jnp.where(causal, m, 0.0).astype(BF16)
        out = jnp.dot(inputs_of(k), m, preferred_element_type=F32)
        r.y[2 * k] = out[:, :128]
        r.y[2 * k + 1] = out[:, 128:]
        return 0

    def inside_part(n):
        cuts = (0, 10, 16)
        lax.fori_loop(cuts[n], cuts[n + 1], inside, 0, unroll=2)

    vr, vi = comm(ar, ai, vr, vi, e_all, inside_part)
    lax.fori_loop(0, CH, functools.partial(advance, keep=True), (vr, vi, one), unroll=8)

    def outputs(k, _):
        at = pl.ds(k, CH, stride=PAIRS)
        v = jnp.concatenate([r.sr[at, :], r.si[at, :]], axis=1).astype(BF16)
        out = lax.dot_general(v, r.qb[k], NT, preferred_element_type=F32)
        r.y[2 * k] += out[:, :128]
        r.y[2 * k + 1] += out[:, 128:]
        return 0

    lax.fori_loop(0, PAIRS, outputs, 0, unroll=2)


def finish_rows(r, q, slot):
    rows = pl.ds(pl.multiple_of(q * 128, 128), 128)

    def turn(j, _):
        parts = block_swap([r.y[j * 8 + n, pl.ds(pl.multiple_of(q * 16, 16), 16), :] for n in range(8)])
        for n in range(8):
            r.v[j, pl.ds(q * 128 + n, 16, stride=8), :] = parts[n]
        return 0

    def close(j, _):
        lanes = pl.ds(pl.multiple_of(j * 128, 128), 128)
        mixed = r.v[j, rows, :] * r.ex[rows, lanes] + r.skip[:, lanes] * r.u[rows, lanes].astype(F32)
        r.act[rows, lanes] = jax.nn.gelu(mixed).astype(BF16)
        return 0

    lax.fori_loop(0, 4, turn, 0, unroll=2)
    lax.fori_loop(0, 4, close, 0, unroll=2)


def fold(acc, vr, vi, e, wr, wi, use):
    er, ei = cmul(wr * e, wi * e, acc[0], acc[1])
    return jnp.where(use, er + vr, acc[0]), jnp.where(use, ei + vi, acc[1]), jnp.where(use, acc[2] * e, acc[2])


def squared(w, times):
    for _ in range(times):
        w = cmul(*w, *w)
    return w


class Refs:
    def __init__(self, **named):
        self.__dict__.update(named)


MIXER_SCRATCH = dict(
    steps=pltpu.VMEM((32, 64), F32), fac=pltpu.VMEM((2, PAIRS, 128), F32), pw=pltpu.VMEM((4, PAIRS * Q, 128), F32), ex=pltpu.VMEM((512, 512), F32), v=pltpu.VMEM((4, 512, 128), F32),
    e7=pltpu.VMEM((CH * PAIRS, 128), F32), z=pltpu.VMEM((32, CH, 128), F32), y=pltpu.VMEM((32, CH, 128), F32),
    pb=pltpu.VMEM((PAIRS, 256, 256), BF16), qb=pltpu.VMEM((PAIRS, 256, 256), BF16),
    sr=pltpu.VMEM((CH * PAIRS, 128), F32), si=pltpu.VMEM((CH * PAIRS, 128), F32),
)


EXCHANGE_SCRATCH = dict(
    mine=pltpu.VMEM((2, 3, PAIRS, 128), F32), got_p=pltpu.VMEM((7, 3, PAIRS, 128), F32),
    got_z=pltpu.VMEM((7, 3, PAIRS, 128), F32), ssem=pltpu.SemaphoreType.DMA((14,)), rsem=pltpu.SemaphoreType.DMA((14,)),
)


def in_plane(n):
    n = lax.rem(n, 8)
    return {"sp_1": n // 2, "sp_2": lax.rem(n, 2)}


def greet(peers):
    barrier = pltpu.get_barrier_semaphore()
    for peer in peers:
        pl.semaphore_signal(barrier, inc=1, device_id=peer, device_id_type=MESH)
    return lambda: pl.semaphore_wait(barrier, len(peers))


def exchange(r, after_own, after_inside, after_plane, after_z, ar, ai, vr, vi, e, part):
    at, z = lax.axis_index("sp_1") * 2 + lax.axis_index("sp_2"), lax.axis_index("sp_0")

    def copy(level, d, got, peer):
        n = level * 7 + d - 1
        return pltpu.make_async_remote_copy(
            src_ref=r.mine.at[level], dst_ref=got.at[d - 1], send_sem=r.ssem.at[n], recv_sem=r.rsem.at[n],
            device_id=peer, device_id_type=MESH,
        )

    def put(level, parts):
        for n, v in enumerate(parts):
            r.mine[level, n] = v

    def of(got, d):
        return got[d - 1, 0], got[d - 1, 1], got[d - 1, 2]

    nothing = (jnp.zeros_like(vr), jnp.zeros_like(vr), jnp.ones_like(vr))
    w1 = squared((ar, ai), 9)
    w8 = squared(w1, 3)
    own = (vr, vi, e)
    put(0, own)
    plane = [copy(0, d, r.got_p, in_plane(at + d)) for d in range(1, 8)]
    for d in (4, 3, 5, 2, 6, 1, 7):
        plane[d - 1].start()
    after_own()
    part(0)
    after_inside()
    for c in plane:
        c.wait()
    total = nothing
    for d in range(7, 0, -1):
        total = fold(total, *of(r.got_p, d), *w1, d <= at)
    total = fold(total, *own, *w1, True)
    for d in range(7, 0, -1):
        total = fold(total, *of(r.got_p, d), *w1, d > at)
    put(1, total)
    sends = [copy(1, d, r.got_z, {"sp_0": lax.rem(z + d, 8)}) for d in range(1, 8)]
    for d in range(1, 8):
        pl.when(z + d < 8)(sends[d - 1].start)
    after_plane()
    part(1)
    after_z()
    for d in range(1, 8):
        pl.when(z + d < 8)(sends[d - 1].wait_send)
        pl.when(z >= d)(sends[d - 1].wait_recv)
    enter = nothing
    for d in range(7, 0, -1):
        enter = fold(enter, *of(r.got_z, d), *w8, d <= z)
    for d in range(7, 0, -1):
        enter = fold(enter, *of(r.got_p, d), *w1, d <= at)
    return enter[0], enter[1]


class Ring:
    def __init__(self, axis, count, many, chunk, others, sent, rsem, swap=False, shared=None):
        self.axis, self.count, self.many, self.chunk, self.others, self.sent, self.rsem = axis, count, many, chunk, others, sent, rsem
        self.swap, self.shared = swap, shared
        self.me, self.half = lax.axis_index(axis), count // 2

    def place(self, steps):
        return lax.rem(self.me + steps + self.count, self.count)

    def moves(self, step, i):
        for way in (0, 1):
            j = i ^ way if self.swap else i
            if step < self.half or (step == self.half and j % 2 == way):
                yield way, j

    def copy(self, step, way, j, owner):
        n = ((step - 1) * 2 + way) * self.many + j
        ref = self.chunk(self.place(owner), j)
        return pltpu.make_async_remote_copy(
            src_ref=ref, dst_ref=ref, send_sem=self.sent, recv_sem=self.rsem.at[n],
            device_id={self.axis: self.place(1 - 2 * way)}, device_id_type=MESH,
        )

    def to_partner(self, ref):
        return pltpu.make_async_remote_copy(
            src_ref=ref, dst_ref=ref, send_sem=self.shared.at[0], recv_sem=self.shared.at[1],
            device_id={"sp_2": 1 - lax.axis_index("sp_2")}, device_id_type=MESH,
        )

    def start(self, i):
        for way, j in self.moves(1, i):
            self.copy(1, way, j, 0).start()

    def service(self, step, i):
        onward = list(self.moves(step + 1, i))
        for way, j in self.moves(step, i):
            self.copy(step, way, j, (2 * way - 1) * step).wait_recv()
            if (way, j) in onward:
                self.copy(step + 1, way, j, (2 * way - 1) * step).start()
            if self.shared is not None:
                self.to_partner(self.chunk(self.place((2 * way - 1) * step), j)).start()

    def shared_wait(self):
        self.to_partner(self.others).wait_recv()

    def drain(self):
        pltpu.make_async_remote_copy(
            src_ref=self.others, dst_ref=self.others, send_sem=self.sent, recv_sem=self.rsem.at[0],
            device_id={self.axis: self.place(1)}, device_id_type=MESH,
        ).wait_send()
        if self.shared is not None:
            self.to_partner(self.others).wait_send()


class RowSum:
    def __init__(self, part, far, near, own, sent, rsem, prepare, quarter):
        self.part, self.far, self.near, self.own, self.sent, self.rsem = part, far, near, own, sent, rsem
        self.y, self.prepare, self.quarter = lax.axis_index("tp"), prepare, quarter
        self.fars = [self.copy(n, part.at[0, n], far.at[n], 1 if n < 2 else 3) for n in range(4)]
        self.nears = [
            self.copy(4, part.at[1, pl.ds(2, 2)], near.at[0, pl.ds(2, 2)], 1), self.copy(5, part.at[2, pl.ds(0, 2)], near.at[1, pl.ds(0, 2)], 3)
        ]
        self.sums = [self.copy(6 + n, part.at[1 + n // 2, n], near.at[n // 2, n], 1 if n < 2 else 3) for n in range(4)]

    def copy(self, n, src, dst, d):
        return pltpu.make_async_remote_copy(
            src_ref=src, dst_ref=dst, send_sem=self.sent, recv_sem=self.rsem.at[n],
            device_id={"tp": lax.rem(self.y + d, 4)}, device_id_type=MESH,
        )

    def make(self, slot, d, *order):
        for n in order:
            self.part[slot, n] = self.quarter(lax.rem(self.y + d, 4), n, slot).astype(BF16)

    def others(self, busy):
        self.prepare(lax.rem(self.y + 2, 4), 0)
        for pair in ((0, 2), (1, 3)):
            self.make(0, 2, *pair)
            for n in pair:
                self.fars[n].start()
        busy(0)
        self.prepare(lax.rem(self.y + 1, 4), 1)
        self.make(1, 1, 2, 3)
        self.nears[0].start()
        busy(1)
        self.prepare(lax.rem(self.y + 3, 4), 2)
        self.make(2, 3, 0, 1)
        self.nears[1].start()
        self.make(2, 3, 2, 3)
        self.make(1, 1, 0, 1)
        busy(2)

    def mine(self):
        self.prepare(self.y, 3)
        for n in range(4):
            self.own[n] = self.quarter(self.y, n, 3)

    def pass_on(self):
        for n in (0, 2, 1, 3):
            self.fars[n].wait_recv()
            slot = 1 + n // 2
            self.part[slot, n] = (self.part[slot, n].astype(F32) + self.far[n].astype(F32)).astype(BF16)
            self.sums[n].start()

    def arrived(self):
        for c in self.nears + self.sums:
            c.wait_recv()

    def total(self, n, at):
        return self.own[n][at] + self.near[0, n][at].astype(F32) + self.near[1, n][at].astype(F32)

    def drain(self):
        self.copy(0, self.part, self.part, 1).wait_send()


def sems(n):
    return pltpu.SemaphoreType.DMA((n,))


IN_VMEM = dict(
    u=((512, 512), BF16), damp=((32, 512), F32), ls=((1, 32), F32), rr=((32, 64), F32), ri=((32, 64), F32), inm=((2, 32, 16, 64), F32),
    outm=((2, 32, 16, 64), F32), skip=((1, 512), F32), residual=((128, 2048), BF16), gain=((1, 2048), F32), taps=((3, 2, 1408), F32),
    w_out=((512, 2048), BF16),
)
EARLY = ("u", "damp", "ls", "rr", "ri", "inm", "outm", "skip")
WEIGHTS = ("w_act", "w_lin", "w_dn")
LAYER_SCRATCH = dict(
    act=pltpu.VMEM((512, 512), BF16), g=pltpu.VMEM((3, 8, 4, 2, 32, 1408), BF16), load=sems(4), result=pltpu.VMEM((128, 2048), BF16),
    stream=pltpu.VMEM((128, 2048), BF16), normed=pltpu.VMEM((33, 16, 2048), BF16),
    pre=pltpu.VMEM((2, 528, 1408), BF16), hidden=pltpu.VMEM((3, 128, 1408), BF16),
    part1=pltpu.VMEM((3, 4, 128, 512), BF16), far1=pltpu.VMEM((4, 128, 512), BF16), near1=pltpu.VMEM((2, 4, 128, 512), BF16),
    own1=pltpu.VMEM((4, 128, 512), F32), sum1_r=sems(10),
    part2=pltpu.VMEM((3, 4, 512, 128), BF16), far2=pltpu.VMEM((4, 512, 128), BF16), near2=pltpu.VMEM((2, 4, 512, 128), BF16),
    own2=pltpu.VMEM((4, 512, 128), F32), sum2_r=sems(10),
    sent=sems(7), ax_r=sems(8), bz_r=sems(16), az_r=sems(32), bx_r=sems(32), ny_r=sems(8), azp=sems(2), bxp=sems(2),
    half_s=sems(2), half_r=sems(2), halo_s=sems(4), halo_r=sems(1),
)
SCRATCH = {**MIXER_SCRATCH, **EXCHANGE_SCRATCH, **LAYER_SCRATCH}


def layer_kernel(*refs):
    given = dict(zip((*IN_VMEM, *WEIGHTS), refs))
    target = refs[len(given)]
    scratch = refs[len(given) + 1 :]
    r = Refs(**dict(zip(IN_VMEM, scratch)), **dict(zip(SCRATCH, scratch[len(IN_VMEM) :])))
    core, x, z, y = (lax.axis_index(a) for a in ("sp_2", "sp_1", "sp_0", "tp"))
    at = z * 8 + x * 2 + core

    def position(n, tp):
        n = lax.rem(n, 64)
        return {"sp_0": n // 8, "sp_1": lax.rem(n, 8) // 2, "sp_2": lax.rem(n, 2), "tp": tp}

    loads = [pltpu.make_async_copy(given[name], getattr(r, name), r.load.at[0 if name in EARLY else 1]) for name in IN_VMEM]
    weights = [pltpu.make_async_copy(given[w], r.g.at[m, z, x, core], r.load.at[2]) for m, w in enumerate(WEIGHTS)]
    for c in loads[: len(EARLY)] + weights + loads[len(EARLY) :]:
        c.start()
    r.got_z[...] = jnp.zeros_like(r.got_z)
    @pl.when(at == 0)
    def _():
        r.normed[0] = jnp.zeros((16, 2048), BF16)

    peers = [in_plane(x * 2 + core + d) for d in range(1, 8)]
    peers += [{axis: lax.rem(lax.axis_index(axis) + d, count)} for axis, count in (("sp_0", 8), ("tp", 4)) for d in range(1, count)]
    peers += [position(at + n, q) for n in (1, 63) for q in range(4)]
    wait_for_all = greet(peers)
    for c in loads[: len(EARLY)]:
        c.wait()

    a_cols, b_cols = pl.ds(0, 640), pl.ds(640, 768)
    a_half, b_half = (pl.ds(0, 384), pl.ds(384, 256)), (pl.ds(640, 384), pl.ds(1024, 384))
    beside_x = [lax.rem(x + n, 4) for n in (0, 1, 3, 2)]
    beside_z = [lax.rem(z + n, 8) for n in (0, 1, 7, 2, 6, 3, 5, 4)]
    ax = Ring("sp_1", 4, 2, lambda o, j: r.g.at[:, z, o, core, :, a_half[j]], r.g.at[:, z, pl.ds(0, 3), core, :, a_cols], r.sent.at[0], r.ax_r, True)
    bz = Ring("sp_0", 8, 2, lambda o, j: r.g.at[:, o, x, core, :, b_half[j]], r.g.at[:, pl.ds(0, 7), x, core, :, b_cols], r.sent.at[1], r.bz_r, True)
    az = Ring("sp_0", 8, 4, lambda o, j: r.g.at[:, o, beside_x[j], core, :, a_cols], r.g.at[:, pl.ds(0, 7), :, core, :, a_cols], r.sent.at[2], r.az_r, False, r.azp)
    bx = Ring("sp_1", 4, 8, lambda o, j: r.g.at[:, beside_z[j], o, core, :, b_cols], r.g.at[:, :, pl.ds(0, 3), core, :, b_cols], r.sent.at[3], r.bx_r, False, r.bxp)
    ny = Ring("tp", 4, 2, lambda o, j: r.normed.at[pl.ds(1 + o * 8 + j * 4, 4)], r.normed.at[pl.ds(0, 24)], r.sent.at[4], r.ny_r, True)

    def half_copies(c):
        return [
            pltpu.make_async_remote_copy(
                src_ref=ref, dst_ref=ref, send_sem=r.half_s.at[n], recv_sem=r.half_r.at[n], device_id={"sp_2": 1 - core}, device_id_type=MESH
            )
            for n, ref in enumerate((r.g.at[:, z, :, c, :, a_cols], r.g.at[:, :, x, c, :, b_cols]))
        ]

    def serve(*steps):
        for ring, step, i in steps:
            ring.service(step, i)

    def greeted():
        for c in weights:
            c.wait()
        wait_for_all()
        for i in (0, 1):
            ax.start(i)
            bz.start(i)
        az.start(0)

    def after_inside():
        serve((ax, 1, 0), (ax, 1, 1), (bz, 1, 0), (bz, 1, 1))

    def after_plane():
        for j in (1, 2):
            az.start(j)
            bx.start(j)

    def after_z():
        serve((ax, 2, 0))
        az.start(3)
        serve((az, 1, 0))

    mixer_phase(r, greeted, functools.partial(exchange, r, lambda: bx.start(0), after_inside, after_plane, after_z))

    for c in loads[len(EARLY) :]:
        c.wait()

    def project(b, n, slot):
        rows = pl.ds(pl.multiple_of(b * 128, 128), 128)
        return jnp.dot(r.act[rows, :], r.w_out[:, pl.ds(n * 512, 512)], preferred_element_type=F32)

    def while_projecting(slot):
        if slot == 0:
            serve((bz, 2, 0), (bz, 2, 1))
            bx.start(3)
            bx.start(4)
        elif slot == 1:
            serve((bx, 1, 0))

    first = RowSum(r.part1, r.far1, r.near1, r.own1, r.sent.at[5], r.sum1_r, functools.partial(finish_rows, r), project)
    first.others(while_projecting)
    first.mine()
    serve((az, 1, 1), (bx, 1, 1))
    first.pass_on()
    serve((az, 1, 2), (bx, 1, 2), (bz, 3, 0), (bz, 3, 1))
    bx.start(5)
    bx.start(6)
    serve((az, 1, 3), (bx, 2, 0), (az, 2, 0), (bx, 1, 3), (bx, 2, 1), (az, 2, 1), (bx, 1, 4), (bz, 4, 0))
    bx.start(7)
    for c in half_copies(core):
        c.start()
    first.arrived()

    def add_up(n, squares):
        cols = pl.ds(pl.multiple_of(n * 512, 512), 512)
        total = r.residual[:, cols].astype(F32) + first.total(n, ...)
        total = total.astype(BF16)
        r.stream[:, cols] = total
        total = total.astype(F32)
        return squares + total * total

    squares = lax.fori_loop(0, 4, add_up, jnp.zeros((128, 512), F32))
    scale = lax.rsqrt(jnp.sum(squares, axis=1, keepdims=True) / 2048 + 1e-06)

    def normalize(n, _):
        cols = pl.ds(pl.multiple_of(n * 256, 256), 256)
        v = (r.stream[:, cols].astype(F32) * scale * r.gain[:, cols]).astype(BF16)
        r.normed[pl.ds(1 + 8 * y, 8), :, cols] = v.reshape(8, 16, 256)
        return 0

    lax.fori_loop(0, 8, normalize, 0)
    ny.start(0)
    ny.start(1)
    halos = [
        pltpu.make_async_remote_copy(
            src_ref=r.normed.at[32], dst_ref=r.normed.at[0], send_sem=r.halo_s.at[q], recv_sem=r.halo_r.at[0],
            device_id=position(at + 1, q), device_id_type=MESH,
        )
        for q in range(4)
    ]
    ends = jnp.logical_and(y == 3, at < 63)

    @pl.when(ends)
    def _():
        for c in halos:
            c.start()

    serve((az, 2, 2), (bx, 2, 2), (az, 2, 3), (bx, 2, 3), (bx, 1, 5), (az, 3, 0), (bx, 2, 4), (bx, 1, 6), (az, 3, 1), (ny, 1, 0))
    serve((az, 3, 2), (bx, 1, 7), (bx, 2, 5), (az, 3, 3), (bx, 2, 6), (az, 4, 0), (az, 4, 1), (bx, 2, 7), (az, 4, 2), (az, 4, 3))
    for c in half_copies(1 - core):
        c.wait_recv()
    bx.shared_wait()
    az.shared_wait()
    pl.when(at > 0)(halos[0].wait_recv)
    serve((ny, 1, 1), (ny, 2, 0))

    def up(w):
        return jnp.dot(r.normed[...].reshape(528, 2048), w, preferred_element_type=F32).astype(BF16)

    def up_tile(n, _):
        m, cols = n % 2, pl.ds(pl.multiple_of((n // 2) * 256, 256), 256)
        r.pre[m, :, cols] = up(r.g[m, :, :, :, :, cols].reshape(2048, 256))
        return 0

    lax.fori_loop(0, 10, up_tile, 0, unroll=2)
    tail = pl.ds(1280, 128)
    last = up(jnp.concatenate([r.g[m, :, :, :, :, tail].reshape(2048, 128) for m in (0, 1)], axis=1))
    r.pre[0, :, tail], r.pre[1, :, tail] = last[:, :128], last[:, 128:]

    def convolved(b, m, cols):
        v = r.pre[m, pl.ds(pl.multiple_of(b * 128, 128), 144), cols].astype(F32)
        return sum(r.taps[k, pl.ds(m, 1), cols] * v[14 + k : 142 + k] for k in range(3))

    def hide(b, slot):
        def tile(n, _):
            cols = pl.ds(pl.multiple_of(n * 128, 128), 128)
            a, l = convolved(b, 0, cols), convolved(b, 1, cols)
            r.hidden[slot % 3, :, cols] = (a / (1.0 + jnp.exp(-a)) * l).astype(BF16)
            return 0

        lax.fori_loop(0, 11, tile, 0)

    def down(b, n, slot):
        w = r.g[2, pl.ds(2 * n, 2)].reshape(512, 1408)
        return lax.dot_general(w, r.hidden[slot % 3], NT, preferred_element_type=F32)

    second = RowSum(r.part2, r.far2, r.near2, r.own2, r.sent.at[6], r.sum2_r, hide, down)
    second.others(lambda slot: None)
    second.pass_on()
    second.mine()
    second.arrived()

    results = []
    for n in range(4):
        cols = pl.ds(n * 512, 512)
        total = jnp.transpose(second.total(n, ...))
        r.result[:, cols] = (r.stream[:, cols].astype(F32) + total).astype(BF16)
        results.append(pltpu.make_async_copy(r.result.at[:, cols], target.at[:, cols], r.load.at[3]))
        results[-1].start()
    for ring in (ax, bz, az, bx, ny):
        ring.drain()
    for c in half_copies(core):
        c.wait_send()
    first.drain()
    second.drain()

    @pl.when(ends)
    def _():
        for c in halos:
            c.wait_send()

    for c in results:
        c.wait()


def per_device(
    mixer_input, residual, log_step, rate_real, rate_imag, damping, in_map, out_map, skip, w_out, norm_gain, w_act, w_lin, conv_taps, w_down
):
    given = (
        mixer_input, damping.T, log_step[None], rate_real, rate_imag, in_map.transpose(0, 1, 3, 2), out_map, skip[None], residual,
        norm_gain[None], conv_taps.transpose(1, 0, 2), w_out, w_act, w_lin, w_down.T,
    )
    return pl.pallas_call(
        layer_kernel,
        out_shape=jax.ShapeDtypeStruct(residual.shape, BF16),
        in_specs=[pl.BlockSpec(memory_space=pl.ANY)] * len(given),
        out_specs=pl.BlockSpec(memory_space=pl.ANY),
        scratch_shapes=[pltpu.VMEM(*v) for v in IN_VMEM.values()] + list(SCRATCH.values()),
        compiler_params=pltpu.CompilerParams(collective_id=0, has_side_effects=True, vmem_limit_bytes=60 * 2**20),
        name="layer",
    )(*given)


def solution(mesh):
    split = Mesh(mesh.devices.reshape(8, 4, 2, mesh.shape["tp"]), ("sp_0", "sp_1", "sp_2", "tp"))
    in_specs = (
        P(SP, "tp"),
        P(SP_TP, None),
        P("tp"),
        P("tp", None),
        P("tp", None),
        P(SP, "tp"),
        P(None, "tp", None, None),
        P(None, "tp", None, None),
        P("tp"),
        P("tp", None),
        P(),
        P(SP, "tp"),
        P(SP, "tp"),
        P(None, None, "tp"),
        P("tp", SP),
    )
    out_specs = P(SP_TP, None)
    return jax.shard_map(
        per_device, mesh=split, in_specs=in_specs, out_specs=out_specs, check_vma=False
    )
```

```python
import functools

import jax
import jax.numpy as jnp
from jax import lax
from jax.experimental import pallas as pl
from jax.experimental.pallas import tpu as pltpu
from jax.sharding import Mesh
from jax.sharding import PartitionSpec as P

F32, BF16 = jnp.float32, jnp.bfloat16
NT = (((1,), (1,)), ((), ()))
TN = (((0,), (0,)), ((), ()))
Q, CH, PAIRS = 8, 64, 16
SP = ("sp_0", "sp_1", "sp_2")
SP_TP = ("sp_0", "sp_1", "sp_2", "tp")
MESH = pl.DeviceIdType.MESH

def iota(shape, dim):
    return lax.broadcasted_iota(jnp.int32, shape, dim)

def cmul(ar, ai, br, bi):
    return ar * br - ai * bi, ar * bi + ai * br

def split3(x):
    hi = x.astype(BF16)
    r = x - hi.astype(F32)
    mid = r.astype(BF16)
    lo = (r - mid.astype(F32)).astype(BF16)
    return hi, mid, lo

def block_swap(parts):
    parts = list(parts)
    block = iota(parts[0].shape, 1) // 16
    for b in (4, 2, 1):
        here = (block // b) % 2 == 0
        for n in range(8):
            if n & b == 0:
                low, high = parts[n], parts[n + b]
                parts[n] = jnp.where(here, low, pltpu.roll(high, 16 * b, axis=1))
                parts[n + b] = jnp.where(here, pltpu.roll(low, 128 - 16 * b, axis=1), high)
    return parts


def paired(even, odd):
    return jnp.concatenate([even, odd], axis=1)


def mixer_phase(r, greeted, comm):
    def rows(ref):
        return paired(ref[pl.ds(0, PAIRS, stride=2), :], ref[pl.ds(1, PAIRS, stride=2), :])

    square = iota((32, 32), 0) == iota((32, 32), 1)
    r.steps[...] = jnp.broadcast_to(jnp.sum(jnp.where(square, r.ls[...], 0.0), axis=1, keepdims=True), (32, 64))
    rr, ri = rows(r.rr), rows(r.ri)
    step = jnp.exp(rows(r.steps))
    lr, th = rr * step, ri * step
    cos, sin = jnp.cos(th), jnp.sin(th)
    mag, inv = jnp.exp(lr), jnp.exp(-lr)
    ar, ai = mag * cos, mag * sin
    den = rr * rr + ri * ri
    r.fac[0] = ((ar - 1.0) * rr + ai * ri) / den
    r.fac[1] = (ai * rr - (ar - 1.0) * ri) / den
    one, zero = jnp.ones_like(ar), jnp.zeros_like(ar)
    pr, pi, nr, ni = one, zero, one, zero
    for s in range(Q):
        at = pl.ds(s, PAIRS, stride=Q)
        r.pw[0, at, :], r.pw[1, at, :] = nr, ni
        r.pw[2, at, :], r.pw[3, at, :] = pr, pi
        pr, pi = cmul(pr, pi, ar, ai)
        nr, ni = cmul(nr, ni, inv * cos, -inv * sin)
    d = r.damp[...]
    lane = iota(d.shape, 1) % Q
    for sh in (1, 2, 4):
        d = d + jnp.where(lane >= sh, pltpu.roll(d, sh, axis=1), 0.0)
    ex = (iota((96, 512), 0) % 32 == iota((96, 512), 1) // 16).astype(F32).astype(BF16)
    def spread_out(v):
        parts = jnp.concatenate([p.astype(F32) for p in split3(v)], axis=0).astype(BF16)
        return lax.dot_general(parts, ex, TN, preferred_element_type=F32)

    pick = (iota((CH, 512), 1) == Q * iota((CH, 512), 0) + Q - 1).astype(F32).astype(BF16)
    ends = sum(lax.dot_general(pick, p, NT, preferred_element_type=F32) for p in split3(d))
    ends = jnp.exp(ends)
    low = iota((CH, 128), 1) < 64
    for k in range(PAIRS):
        r.e7[pl.ds(k, CH, stride=PAIRS), :] = jnp.where(low, ends[:, 2 * k : 2 * k + 1], ends[:, 2 * k + 1 : 2 * k + 2])

    r.ex[...] = spread_out(jnp.exp(d))
    shrink = spread_out(jnp.exp(-d)) * r.u[...].astype(F32)
    for j in range(4):
        r.v[j] = shrink[:, j * 128 : j * 128 + 128]

    def spread(b, _):
        j, c = b // 2, b % 2
        parts = block_swap([r.v[j, pl.ds(c * 256 + n, 32, stride=8), :] for n in range(8)])
        for n in range(8):
            r.z[j * 8 + n, pl.ds(pl.multiple_of(c * 32, 32), 32), :] = parts[n]
        return 0

    lax.fori_loop(0, 8, spread, 0)
    greeted()

    low = iota((128, 128), 1) < 64

    def stacked(re, im):
        top = jnp.concatenate([jnp.where(low, re, 0.0), jnp.where(low, im, 0.0)], axis=1)
        bottom = jnp.concatenate([jnp.where(low, 0.0, re), jnp.where(low, 0.0, im)], axis=1)
        return jnp.concatenate([top, bottom], axis=0).astype(BF16)

    def outer(which, k, br, bi):
        at = pl.ds(pl.multiple_of(k * Q, Q), Q)
        wr, wi = r.pw[which, at, :][:, None, :], r.pw[which + 1, at, :][:, None, :]
        br, bi = br[None], bi[None]
        re, im = cmul(wr, wi, br, bi)
        return re.reshape(128, 128), im.reshape(128, 128)

    def inputs_of(k):
        return jnp.concatenate([r.z[2 * k], r.z[2 * k + 1]], axis=1).astype(BF16)

    def states_in(k, _):
        br, bi = paired(r.inm[0, 2 * k], r.inm[0, 2 * k + 1]), paired(r.inm[1, 2 * k], r.inm[1, 2 * k + 1])
        br, bi = cmul(r.fac[0, pl.ds(k, 1), :], r.fac[1, pl.ds(k, 1), :], br, bi)
        p = stacked(*outer(0, k, br, bi))
        r.pb[k] = p
        s = jnp.dot(inputs_of(k), p, preferred_element_type=F32)
        at = pl.ds(k, CH, stride=PAIRS)
        r.sr[at, :] = s[:, :128]
        r.si[at, :] = s[:, 128:]
        return 0

    lax.fori_loop(0, PAIRS, states_in, 0, unroll=2)

    a2r, a2i = cmul(ar, ai, ar, ai)
    a4r, a4i = cmul(a2r, a2i, a2r, a2i)
    a8r, a8i = cmul(a4r, a4i, a4r, a4i)

    def advance(c, carry, keep):
        vr, vi, e_all = carry
        at = pl.ds(pl.multiple_of(c * PAIRS, PAIRS), PAIRS)
        e = r.e7[at, :]
        tr, ti = (vr + r.sr[at, :]) * e, (vi + r.si[at, :]) * e
        if keep:
            r.sr[at, :], r.si[at, :] = vr, vi
        vr, vi = cmul(a8r, a8i, tr, ti)
        return vr, vi, e_all * e

    vr, vi, e_all = lax.fori_loop(0, CH, functools.partial(advance, keep=False), (zero, zero, one), unroll=8)

    causal = (iota((256, 256), 0) // 16) % Q <= (iota((256, 256), 1) // 16) % Q

    def inside(k, _):
        cr, ci = paired(r.outm[0, 2 * k], r.outm[0, 2 * k + 1]), paired(r.outm[1, 2 * k], r.outm[1, 2 * k + 1])
        qr, qi = outer(2, k, cr, ci)
        q = stacked(qr, -qi)
        r.qb[k] = q
        m = lax.dot_general(r.pb[k], q, NT, preferred_element_type=F32)
        m = jnp.where(causal, m, 0.0).astype(BF16)
        out = jnp.dot(inputs_of(k), m, preferred_element_type=F32)
        r.y[2 * k] = out[:, :128]
        r.y[2 * k + 1] = out[:, 128:]
        return 0

    def inside_part(n):
        cuts = (0, 10, 16)
        lax.fori_loop(cuts[n], cuts[n + 1], inside, 0, unroll=2)

    vr, vi = comm(ar, ai, vr, vi, e_all, inside_part)
    lax.fori_loop(0, CH, functools.partial(advance, keep=True), (vr, vi, one), unroll=8)

    def outputs(k, _):
        at = pl.ds(k, CH, stride=PAIRS)
        v = jnp.concatenate([r.sr[at, :], r.si[at, :]], axis=1).astype(BF16)
        out = lax.dot_general(v, r.qb[k], NT, preferred_element_type=F32)
        r.y[2 * k] += out[:, :128]
        r.y[2 * k + 1] += out[:, 128:]
        return 0

    lax.fori_loop(0, PAIRS, outputs, 0, unroll=2)


def finish_rows(r, q, slot):
    rows = pl.ds(pl.multiple_of(q * 128, 128), 128)

    def turn(j, _):
        parts = block_swap([r.y[j * 8 + n, pl.ds(pl.multiple_of(q * 16, 16), 16), :] for n in range(8)])
        for n in range(8):
            r.v[j, pl.ds(q * 128 + n, 16, stride=8), :] = parts[n]
        return 0

    def close(j, _):
        lanes = pl.ds(pl.multiple_of(j * 128, 128), 128)
        mixed = r.v[j, rows, :] * r.ex[rows, lanes] + r.skip[:, lanes] * r.u[rows, lanes].astype(F32)
        r.act[rows, lanes] = jax.nn.gelu(mixed).astype(BF16)
        return 0

    lax.fori_loop(0, 4, turn, 0, unroll=2)
    lax.fori_loop(0, 4, close, 0, unroll=2)


def fold(acc, vr, vi, e, wr, wi, use):
    er, ei = cmul(wr * e, wi * e, acc[0], acc[1])
    return jnp.where(use, er + vr, acc[0]), jnp.where(use, ei + vi, acc[1]), jnp.where(use, acc[2] * e, acc[2])


def squared(w, times):
    for _ in range(times):
        w = cmul(*w, *w)
    return w


class Refs:
    def __init__(self, **named):
        self.__dict__.update(named)


MIXER_SCRATCH = dict(
    steps=pltpu.VMEM((32, 64), F32), fac=pltpu.VMEM((2, PAIRS, 128), F32), pw=pltpu.VMEM((4, PAIRS * Q, 128), F32), ex=pltpu.VMEM((512, 512), F32), v=pltpu.VMEM((4, 512, 128), F32),
    e7=pltpu.VMEM((CH * PAIRS, 128), F32), z=pltpu.VMEM((32, CH, 128), F32), y=pltpu.VMEM((32, CH, 128), F32),
    pb=pltpu.VMEM((PAIRS, 256, 256), BF16), qb=pltpu.VMEM((PAIRS, 256, 256), BF16),
    sr=pltpu.VMEM((CH * PAIRS, 128), F32), si=pltpu.VMEM((CH * PAIRS, 128), F32),
)


EXCHANGE_SCRATCH = dict(
    mine=pltpu.VMEM((2, 3, PAIRS, 128), F32), got_p=pltpu.VMEM((7, 3, PAIRS, 128), F32),
    got_z=pltpu.VMEM((7, 3, PAIRS, 128), F32), ssem=pltpu.SemaphoreType.DMA((14,)), rsem=pltpu.SemaphoreType.DMA((14,)),
)


def in_plane(n):
    n = lax.rem(n, 8)
    return {"sp_1": n // 2, "sp_2": lax.rem(n, 2)}


def greet(peers):
    barrier = pltpu.get_barrier_semaphore()
    for peer in peers:
        pl.semaphore_signal(barrier, inc=1, device_id=peer, device_id_type=MESH)
    return lambda: pl.semaphore_wait(barrier, len(peers))


def exchange(r, after_own, after_inside, after_plane, after_z, ar, ai, vr, vi, e, part):
    at, z = lax.axis_index("sp_1") * 2 + lax.axis_index("sp_2"), lax.axis_index("sp_0")

    def copy(level, d, got, peer):
        n = level * 7 + d - 1
        return pltpu.make_async_remote_copy(
            src_ref=r.mine.at[level], dst_ref=got.at[d - 1], send_sem=r.ssem.at[n], recv_sem=r.rsem.at[n],
            device_id=peer, device_id_type=MESH,
        )

    def put(level, parts):
        for n, v in enumerate(parts):
            r.mine[level, n] = v

    def of(got, d):
        return got[d - 1, 0], got[d - 1, 1], got[d - 1, 2]

    nothing = (jnp.zeros_like(vr), jnp.zeros_like(vr), jnp.ones_like(vr))
    w1 = squared((ar, ai), 9)
    w8 = squared(w1, 3)
    own = (vr, vi, e)
    put(0, own)
    plane = [copy(0, d, r.got_p, in_plane(at + d)) for d in range(1, 8)]
    for d in (4, 3, 5, 2, 6, 1, 7):
        plane[d - 1].start()
    after_own()
    part(0)
    after_inside()
    for c in plane:
        c.wait()
    total = nothing
    for d in range(7, 0, -1):
        total = fold(total, *of(r.got_p, d), *w1, d <= at)
    total = fold(total, *own, *w1, True)
    for d in range(7, 0, -1):
        total = fold(total, *of(r.got_p, d), *w1, d > at)
    put(1, total)
    sends = [copy(1, d, r.got_z, {"sp_0": lax.rem(z + d, 8)}) for d in range(1, 8)]
    for d in range(1, 8):
        pl.when(z + d < 8)(sends[d - 1].start)
    after_plane()
    part(1)
    after_z()
    for d in range(1, 8):
        pl.when(z + d < 8)(sends[d - 1].wait_send)
        pl.when(z >= d)(sends[d - 1].wait_recv)
    enter = nothing
    for d in range(7, 0, -1):
        enter = fold(enter, *of(r.got_z, d), *w8, d <= z)
    for d in range(7, 0, -1):
        enter = fold(enter, *of(r.got_p, d), *w1, d <= at)
    return enter[0], enter[1]


class Ring:
    def __init__(self, axis, count, many, chunk, others, sent, rsem, swap=False, shared=None):
        self.axis, self.count, self.many, self.chunk, self.others, self.sent, self.rsem = axis, count, many, chunk, others, sent, rsem
        self.swap, self.shared = swap, shared
        self.me, self.half = lax.axis_index(axis), count // 2

    def place(self, steps):
        return lax.rem(self.me + steps + self.count, self.count)

    def moves(self, step, i):
        for way in (0, 1):
            j = i ^ way if self.swap else i
            if step < self.half or (step == self.half and j % 2 == way):
                yield way, j

    def copy(self, step, way, j, owner):
        n = ((step - 1) * 2 + way) * self.many + j
        ref = self.chunk(self.place(owner), j)
        return pltpu.make_async_remote_copy(
            src_ref=ref, dst_ref=ref, send_sem=self.sent, recv_sem=self.rsem.at[n],
            device_id={self.axis: self.place(1 - 2 * way)}, device_id_type=MESH,
        )

    def to_partner(self, ref):
        return pltpu.make_async_remote_copy(
            src_ref=ref, dst_ref=ref, send_sem=self.shared.at[0], recv_sem=self.shared.at[1],
            device_id={"sp_2": 1 - lax.axis_index("sp_2")}, device_id_type=MESH,
        )

    def start(self, i):
        for way, j in self.moves(1, i):
            self.copy(1, way, j, 0).start()

    def service(self, step, i):
        onward = list(self.moves(step + 1, i))
        for way, j in self.moves(step, i):
            self.copy(step, way, j, (2 * way - 1) * step).wait_recv()
            if (way, j) in onward:
                self.copy(step + 1, way, j, (2 * way - 1) * step).start()
            if self.shared is not None:
                self.to_partner(self.chunk(self.place((2 * way - 1) * step), j)).start()

    def shared_wait(self):
        self.to_partner(self.others).wait_recv()

    def drain(self):
        pltpu.make_async_remote_copy(
            src_ref=self.others, dst_ref=self.others, send_sem=self.sent, recv_sem=self.rsem.at[0],
            device_id={self.axis: self.place(1)}, device_id_type=MESH,
        ).wait_send()
        if self.shared is not None:
            self.to_partner(self.others).wait_send()


class RowSum:
    def __init__(self, part, far, near, own, sent, rsem, prepare, quarter):
        self.part, self.far, self.near, self.own, self.sent, self.rsem = part, far, near, own, sent, rsem
        self.y, self.prepare, self.quarter = lax.axis_index("tp"), prepare, quarter
        self.fars = [self.copy(n, part.at[0, n], far.at[n], 1 if n < 2 else 3) for n in range(4)]
        self.nears = [
            self.copy(4, part.at[1, pl.ds(2, 2)], near.at[0, pl.ds(2, 2)], 1), self.copy(5, part.at[2, pl.ds(0, 2)], near.at[1, pl.ds(0, 2)], 3)
        ]
        self.sums = [self.copy(6 + n, part.at[1 + n // 2, n], near.at[n // 2, n], 1 if n < 2 else 3) for n in range(4)]

    def copy(self, n, src, dst, d):
        return pltpu.make_async_remote_copy(
            src_ref=src, dst_ref=dst, send_sem=self.sent, recv_sem=self.rsem.at[n],
            device_id={"tp": lax.rem(self.y + d, 4)}, device_id_type=MESH,
        )

    def make(self, slot, d, *order):
        for n in order:
            self.part[slot, n] = self.quarter(lax.rem(self.y + d, 4), n, slot).astype(BF16)

    def others(self, busy):
        self.prepare(lax.rem(self.y + 2, 4), 0)
        for pair in ((0, 2), (1, 3)):
            self.make(0, 2, *pair)
            for n in pair:
                self.fars[n].start()
        busy(0)
        self.prepare(lax.rem(self.y + 1, 4), 1)
        self.make(1, 1, 2, 3)
        self.nears[0].start()
        busy(1)
        self.prepare(lax.rem(self.y + 3, 4), 2)
        self.make(2, 3, 0, 1)
        self.nears[1].start()
        self.make(2, 3, 2, 3)
        self.make(1, 1, 0, 1)
        busy(2)

    def mine(self):
        self.prepare(self.y, 3)
        for n in range(4):
            self.own[n] = self.quarter(self.y, n, 3)

    def pass_on(self):
        for n in (0, 2, 1, 3):
            self.fars[n].wait_recv()
            slot = 1 + n // 2
            self.part[slot, n] = (self.part[slot, n].astype(F32) + self.far[n].astype(F32)).astype(BF16)
            self.sums[n].start()

    def arrived(self):
        for c in self.nears + self.sums:
            c.wait_recv()

    def total(self, n, at):
        return self.own[n][at] + self.near[0, n][at].astype(F32) + self.near[1, n][at].astype(F32)

    def drain(self):
        self.copy(0, self.part, self.part, 1).wait_send()


def sems(n):
    return pltpu.SemaphoreType.DMA((n,))


IN_VMEM = dict(
    u=((512, 512), BF16), damp=((32, 512), F32), ls=((1, 32), F32), rr=((32, 64), F32), ri=((32, 64), F32), inm=((2, 32, 16, 64), F32),
    outm=((2, 32, 16, 64), F32), skip=((1, 512), F32), residual=((128, 2048), BF16), gain=((1, 2048), F32), taps=((3, 2, 1408), F32),
    w_out=((512, 2048), BF16),
)
EARLY = ("u", "damp", "ls", "rr", "ri", "inm", "outm", "skip")
WEIGHTS = ("w_act", "w_lin", "w_dn")
LAYER_SCRATCH = dict(
    act=pltpu.VMEM((512, 512), BF16), g=pltpu.VMEM((3, 8, 4, 2, 32, 1408), BF16), load=sems(4), result=pltpu.VMEM((128, 2048), BF16),
    stream=pltpu.VMEM((128, 2048), BF16), normed=pltpu.VMEM((33, 16, 2048), BF16),
    pre=pltpu.VMEM((2, 528, 1408), BF16), hidden=pltpu.VMEM((3, 128, 1408), BF16),
    part1=pltpu.VMEM((3, 4, 128, 512), BF16), far1=pltpu.VMEM((4, 128, 512), BF16), near1=pltpu.VMEM((2, 4, 128, 512), BF16),
    own1=pltpu.VMEM((4, 128, 512), F32), sum1_r=sems(10),
    part2=pltpu.VMEM((3, 4, 512, 128), BF16), far2=pltpu.VMEM((4, 512, 128), BF16), near2=pltpu.VMEM((2, 4, 512, 128), BF16),
    own2=pltpu.VMEM((4, 512, 128), F32), sum2_r=sems(10),
    sent=sems(7), ax_r=sems(8), bz_r=sems(16), az_r=sems(32), bx_r=sems(32), ny_r=sems(8), azp=sems(2), bxp=sems(2),
    half_s=sems(2), half_r=sems(2), halo_s=sems(4), halo_r=sems(1),
)
SCRATCH = {**MIXER_SCRATCH, **EXCHANGE_SCRATCH, **LAYER_SCRATCH}


def layer_kernel(*refs):
    given = dict(zip((*IN_VMEM, *WEIGHTS), refs))
    target = refs[len(given)]
    scratch = refs[len(given) + 1 :]
    r = Refs(**dict(zip(IN_VMEM, scratch)), **dict(zip(SCRATCH, scratch[len(IN_VMEM) :])))
    core, x, z, y = (lax.axis_index(a) for a in ("sp_2", "sp_1", "sp_0", "tp"))
    at = z * 8 + x * 2 + core

    def position(n, tp):
        n = lax.rem(n, 64)
        return {"sp_0": n // 8, "sp_1": lax.rem(n, 8) // 2, "sp_2": lax.rem(n, 2), "tp": tp}

    loads = [pltpu.make_async_copy(given[name], getattr(r, name), r.load.at[0 if name in EARLY else 1]) for name in IN_VMEM]
    weights = [pltpu.make_async_copy(given[w], r.g.at[m, z, x, core], r.load.at[2]) for m, w in enumerate(WEIGHTS)]
    for c in loads[: len(EARLY)] + weights + loads[len(EARLY) :]:
        c.start()
    r.got_z[...] = jnp.zeros_like(r.got_z)
    r.normed[0] = jnp.zeros((16, 2048), BF16)
    peers = [in_plane(x * 2 + core + d) for d in range(1, 8)]
    peers += [{axis: lax.rem(lax.axis_index(axis) + d, count)} for axis, count in (("sp_0", 8), ("tp", 4)) for d in range(1, count)]
    peers += [position(at + n, q) for n in (1, 63) for q in range(4)]
    wait_for_all = greet(peers)
    for c in loads[: len(EARLY)]:
        c.wait()

    a_cols, b_cols = pl.ds(0, 640), pl.ds(640, 768)
    a_half, b_half = (pl.ds(0, 384), pl.ds(384, 256)), (pl.ds(640, 384), pl.ds(1024, 384))
    beside_x = [lax.rem(x + n, 4) for n in (0, 1, 3, 2)]
    beside_z = [lax.rem(z + n, 8) for n in (0, 1, 7, 2, 6, 3, 5, 4)]
    ax = Ring("sp_1", 4, 2, lambda o, j: r.g.at[:, z, o, core, :, a_half[j]], r.g.at[:, z, pl.ds(0, 3), core, :, a_cols], r.sent.at[0], r.ax_r, True)
    bz = Ring("sp_0", 8, 2, lambda o, j: r.g.at[:, o, x, core, :, b_half[j]], r.g.at[:, pl.ds(0, 7), x, core, :, b_cols], r.sent.at[1], r.bz_r, True)
    az = Ring("sp_0", 8, 4, lambda o, j: r.g.at[:, o, beside_x[j], core, :, a_cols], r.g.at[:, pl.ds(0, 7), :, core, :, a_cols], r.sent.at[2], r.az_r, False, r.azp)
    bx = Ring("sp_1", 4, 8, lambda o, j: r.g.at[:, beside_z[j], o, core, :, b_cols], r.g.at[:, :, pl.ds(0, 3), core, :, b_cols], r.sent.at[3], r.bx_r, False, r.bxp)
    ny = Ring("tp", 4, 2, lambda o, j: r.normed.at[pl.ds(1 + o * 8 + j * 4, 4)], r.normed.at[pl.ds(0, 24)], r.sent.at[4], r.ny_r, True)

    def half_copies(c):
        return [
            pltpu.make_async_remote_copy(
                src_ref=ref, dst_ref=ref, send_sem=r.half_s.at[n], recv_sem=r.half_r.at[n], device_id={"sp_2": 1 - core}, device_id_type=MESH
            )
            for n, ref in enumerate((r.g.at[:, z, :, c, :, a_cols], r.g.at[:, :, x, c, :, b_cols]))
        ]

    def serve(*steps):
        for ring, step, i in steps:
            ring.service(step, i)

    def greeted():
        for c in weights:
            c.wait()
        wait_for_all()
        for i in (0, 1):
            ax.start(i)
            bz.start(i)
        az.start(0)

    def after_inside():
        serve((ax, 1, 0), (ax, 1, 1), (bz, 1, 0), (bz, 1, 1))

    def after_plane():
        for j in (1, 2):
            az.start(j)
            bx.start(j)

    def after_z():
        serve((ax, 2, 0))
        az.start(3)
        serve((az, 1, 0))

    mixer_phase(r, greeted, functools.partial(exchange, r, lambda: bx.start(0), after_inside, after_plane, after_z))

    for c in loads[len(EARLY) :]:
        c.wait()

    def project(b, n, slot):
        rows = pl.ds(pl.multiple_of(b * 128, 128), 128)
        return jnp.dot(r.act[rows, :], r.w_out[:, pl.ds(n * 512, 512)], preferred_element_type=F32)

    def while_projecting(slot):
        if slot == 0:
            serve((bz, 2, 0), (bz, 2, 1))
            bx.start(3)
            bx.start(4)
        elif slot == 1:
            serve((bx, 1, 0))

    first = RowSum(r.part1, r.far1, r.near1, r.own1, r.sent.at[5], r.sum1_r, functools.partial(finish_rows, r), project)
    first.others(while_projecting)
    first.mine()
    serve((az, 1, 1), (bx, 1, 1))
    first.pass_on()
    serve((az, 1, 2), (bx, 1, 2), (bz, 3, 0), (bz, 3, 1))
    bx.start(5)
    bx.start(6)
    serve((az, 1, 3), (bx, 2, 0), (az, 2, 0), (bx, 1, 3), (bx, 2, 1), (az, 2, 1), (bx, 1, 4), (bz, 4, 0))
    bx.start(7)
    for c in half_copies(core):
        c.start()
    first.arrived()

    def add_up(n, squares):
        cols = pl.ds(pl.multiple_of(n * 512, 512), 512)
        total = r.residual[:, cols].astype(F32) + first.total(n, ...)
        total = total.astype(BF16)
        r.stream[:, cols] = total
        total = total.astype(F32)
        return squares + total * total

    squares = lax.fori_loop(0, 4, add_up, jnp.zeros((128, 512), F32))
    scale = lax.rsqrt(jnp.sum(squares, axis=1, keepdims=True) / 2048 + 1e-06)

    def normalize(n, _):
        cols = pl.ds(pl.multiple_of(n * 256, 256), 256)
        v = (r.stream[:, cols].astype(F32) * scale * r.gain[:, cols]).astype(BF16)
        r.normed[pl.ds(1 + 8 * y, 8), :, cols] = v.reshape(8, 16, 256)
        return 0

    lax.fori_loop(0, 8, normalize, 0)
    halos = [
        pltpu.make_async_remote_copy(
            src_ref=r.normed.at[32, pl.ds(8, 8)], dst_ref=r.normed.at[0, pl.ds(8, 8)], send_sem=r.halo_s.at[q], recv_sem=r.halo_r.at[0],
            device_id=position(at + 1, q), device_id_type=MESH,
        )
        for q in range(4)
    ]
    ends = jnp.logical_and(y == 3, at < 63)

    @pl.when(ends)
    def _():
        for c in halos:
            c.start()

    ny.start(0)
    ny.start(1)
    serve((az, 2, 2), (bx, 2, 2), (az, 2, 3), (bx, 2, 3), (bx, 1, 5), (bx, 1, 6), (az, 3, 0), (bx, 2, 4), (bx, 1, 7), (az, 3, 1), (ny, 1, 0))
    serve((bx, 2, 5), (az, 3, 2), (bx, 2, 6), (az, 3, 3), (bx, 2, 7), (az, 4, 0), (az, 4, 1), (az, 4, 2), (az, 4, 3))
    for c in half_copies(1 - core):
        c.wait_recv()
    pl.when(at > 0)(halos[0].wait_recv)
    bx.shared_wait()
    serve((ny, 1, 1), (ny, 2, 0))

    def up(w):
        return jnp.dot(r.normed[...].reshape(528, 2048), w, preferred_element_type=F32).astype(BF16)

    def up_tile(first, n, _):
        m, cols = n % 2, pl.ds(pl.multiple_of(first + (n // 2) * 256, 128), 256)
        r.pre[m, :, cols] = up(r.g[m, :, :, :, :, cols].reshape(2048, 256))
        return 0

    lax.fori_loop(0, 6, functools.partial(up_tile, 640), 0, unroll=2)
    az.shared_wait()
    lax.fori_loop(0, 4, functools.partial(up_tile, 0), 0, unroll=2)
    tail = pl.ds(512, 128)

    def up_tail(m, _):
        r.pre[m, :, tail] = up(r.g[m, :, :, :, :, tail].reshape(2048, 128))
        return 0

    lax.fori_loop(0, 2, up_tail, 0, unroll=2)

    def convolved(b, m, cols):
        v = r.pre[m, pl.ds(pl.multiple_of(b * 128, 128), 144), cols].astype(F32)
        return sum(r.taps[k, pl.ds(m, 1), cols] * v[14 + k : 142 + k] for k in range(3))

    def hide(b, slot):
        def tile(cols):
            a, l = convolved(b, 0, cols), convolved(b, 1, cols)
            r.hidden[slot % 3, :, cols] = (a / (1.0 + jnp.exp(-a)) * l).astype(BF16)

        def pair(n, _):
            for half in (0, 1):
                tile(pl.ds(pl.multiple_of(n * 256 + half * 128, 128), 128))
            return 0

        lax.fori_loop(0, 5, pair, 0)
        tile(pl.ds(1280, 128))

    def down(b, n, slot):
        w = r.g[2, pl.ds(2 * n, 2)].reshape(512, 1408)
        return lax.dot_general(w, r.hidden[slot % 3], NT, preferred_element_type=F32)

    second = RowSum(r.part2, r.far2, r.near2, r.own2, r.sent.at[6], r.sum2_r, hide, down)
    second.others(lambda slot: None)
    second.pass_on()
    second.mine()
    for c in second.nears:
        c.wait_recv()
    results = []
    for n in (0, 2, 1, 3):
        second.sums[n].wait_recv()
        cols = pl.ds(n * 512, 512)
        total = jnp.transpose(second.total(n, ...))
        r.result[:, cols] = (r.stream[:, cols].astype(F32) + total).astype(BF16)
        results.append(pltpu.make_async_copy(r.result.at[:, cols], target.at[:, cols], r.load.at[3]))
        results[-1].start()
    for ring in (ax, bz, az, bx, ny):
        ring.drain()
    for c in half_copies(core):
        c.wait_send()
    first.drain()
    second.drain()

    @pl.when(ends)
    def _():
        for c in halos:
            c.wait_send()

    for c in results:
        c.wait()


def per_device(
    mixer_input, residual, log_step, rate_real, rate_imag, damping, in_map, out_map, skip, w_out, norm_gain, w_act, w_lin, conv_taps, w_down
):
    given = (
        mixer_input, damping.T, log_step[None], rate_real, rate_imag, in_map.transpose(0, 1, 3, 2), out_map, skip[None], residual,
        norm_gain[None], conv_taps.transpose(1, 0, 2), w_out, w_act, w_lin, w_down.T,
    )
    return pl.pallas_call(
        layer_kernel,
        out_shape=jax.ShapeDtypeStruct(residual.shape, BF16),
        in_specs=[pl.BlockSpec(memory_space=pl.ANY)] * len(given),
        out_specs=pl.BlockSpec(memory_space=pl.ANY),
        scratch_shapes=[pltpu.VMEM(*v) for v in IN_VMEM.values()] + list(SCRATCH.values()),
        compiler_params=pltpu.CompilerParams(collective_id=0, has_side_effects=True, vmem_limit_bytes=60 * 2**20),
        name="layer",
    )(*given)


def solution(mesh):
    split = Mesh(mesh.devices.reshape(8, 4, 2, mesh.shape["tp"]), ("sp_0", "sp_1", "sp_2", "tp"))
    in_specs = (
        P(SP, "tp"),
        P(SP_TP, None),
        P("tp"),
        P("tp", None),
        P("tp", None),
        P(SP, "tp"),
        P(None, "tp", None, None),
        P(None, "tp", None, None),
        P("tp"),
        P("tp", None),
        P(),
        P(SP, "tp"),
        P(SP, "tp"),
        P(None, None, "tp"),
        P("tp", SP),
    )
    out_specs = P(SP_TP, None)
    return jax.shard_map(
        per_device, mesh=split, in_specs=in_specs, out_specs=out_specs, check_vma=False
    )
```

```python
import functools

import jax
import jax.numpy as jnp
from jax import lax
from jax.experimental import pallas as pl
from jax.experimental.pallas import tpu as pltpu
from jax.sharding import Mesh
from jax.sharding import PartitionSpec as P

F32, BF16 = jnp.float32, jnp.bfloat16
NT = (((1,), (1,)), ((), ()))
TN = (((0,), (0,)), ((), ()))
Q, CH, PAIRS = 8, 64, 16
SP = ("sp_0", "sp_1", "sp_2")
SP_TP = ("sp_0", "sp_1", "sp_2", "tp")
MESH = pl.DeviceIdType.MESH

def iota(shape, dim):
    return lax.broadcasted_iota(jnp.int32, shape, dim)

def cmul(ar, ai, br, bi):
    return ar * br - ai * bi, ar * bi + ai * br

def split3(x):
    hi = x.astype(BF16)
    r = x - hi.astype(F32)
    mid = r.astype(BF16)
    lo = (r - mid.astype(F32)).astype(BF16)
    return hi, mid, lo

def block_swap(parts):
    parts = list(parts)
    block = iota(parts[0].shape, 1) // 16
    for b in (4, 2, 1):
        here = (block // b) % 2 == 0
        for n in range(8):
            if n & b == 0:
                low, high = parts[n], parts[n + b]
                parts[n] = jnp.where(here, low, pltpu.roll(high, 16 * b, axis=1))
                parts[n + b] = jnp.where(here, pltpu.roll(low, 128 - 16 * b, axis=1), high)
    return parts


def paired(even, odd):
    return jnp.concatenate([even, odd], axis=1)


def mixer_phase(r, greeted, comm):
    def rows(ref):
        return paired(ref[pl.ds(0, PAIRS, stride=2), :], ref[pl.ds(1, PAIRS, stride=2), :])

    square = iota((32, 32), 0) == iota((32, 32), 1)
    r.steps[...] = jnp.broadcast_to(jnp.sum(jnp.where(square, r.ls[...], 0.0), axis=1, keepdims=True), (32, 64))
    rr, ri = rows(r.rr), rows(r.ri)
    step = jnp.exp(rows(r.steps))
    lr, th = rr * step, ri * step
    cos, sin = jnp.cos(th), jnp.sin(th)
    mag, inv = jnp.exp(lr), jnp.exp(-lr)
    ar, ai = mag * cos, mag * sin
    den = rr * rr + ri * ri
    r.fac[0] = ((ar - 1.0) * rr + ai * ri) / den
    r.fac[1] = (ai * rr - (ar - 1.0) * ri) / den
    one, zero = jnp.ones_like(ar), jnp.zeros_like(ar)
    pr, pi, nr, ni = one, zero, one, zero
    for s in range(Q):
        at = pl.ds(s, PAIRS, stride=Q)
        r.pw[0, at, :], r.pw[1, at, :] = nr, ni
        r.pw[2, at, :], r.pw[3, at, :] = pr, pi
        pr, pi = cmul(pr, pi, ar, ai)
        nr, ni = cmul(nr, ni, inv * cos, -inv * sin)
    d = r.damp[...]
    lane = iota(d.shape, 1) % Q
    for sh in (1, 2, 4):
        d = d + jnp.where(lane >= sh, pltpu.roll(d, sh, axis=1), 0.0)
    ex = (iota((96, 512), 0) % 32 == iota((96, 512), 1) // 16).astype(F32).astype(BF16)
    def spread_out(v):
        parts = jnp.concatenate([p.astype(F32) for p in split3(v)], axis=0).astype(BF16)
        return lax.dot_general(parts, ex, TN, preferred_element_type=F32)

    pick = (iota((CH, 512), 1) == Q * iota((CH, 512), 0) + Q - 1).astype(F32).astype(BF16)
    ends = sum(lax.dot_general(pick, p, NT, preferred_element_type=F32) for p in split3(d))
    ends = jnp.exp(ends)
    low = iota((CH, 128), 1) < 64
    for k in range(PAIRS):
        r.e7[pl.ds(k, CH, stride=PAIRS), :] = jnp.where(low, ends[:, 2 * k : 2 * k + 1], ends[:, 2 * k + 1 : 2 * k + 2])

    shrink = spread_out(jnp.exp(-d)) * r.u[...].astype(F32)
    for j in range(4):
        r.v[j] = shrink[:, j * 128 : j * 128 + 128]

    def spread(b, _):
        j, c = b // 2, b % 2
        parts = block_swap([r.v[j, pl.ds(c * 256 + n, 32, stride=8), :] for n in range(8)])
        for n in range(8):
            r.z[j * 8 + n, pl.ds(pl.multiple_of(c * 32, 32), 32), :] = parts[n]
        return 0

    lax.fori_loop(0, 8, spread, 0)
    greeted()

    low = iota((128, 128), 1) < 64

    def stacked(re, im):
        top = jnp.concatenate([jnp.where(low, re, 0.0), jnp.where(low, im, 0.0)], axis=1)
        bottom = jnp.concatenate([jnp.where(low, 0.0, re), jnp.where(low, 0.0, im)], axis=1)
        return jnp.concatenate([top, bottom], axis=0).astype(BF16)

    def outer(which, k, br, bi):
        at = pl.ds(pl.multiple_of(k * Q, Q), Q)
        wr, wi = r.pw[which, at, :][:, None, :], r.pw[which + 1, at, :][:, None, :]
        br, bi = br[None], bi[None]
        re, im = cmul(wr, wi, br, bi)
        return re.reshape(128, 128), im.reshape(128, 128)

    def inputs_of(k):
        return jnp.concatenate([r.z[2 * k], r.z[2 * k + 1]], axis=1).astype(BF16)

    def states_in(k, _):
        br, bi = paired(r.inm[0, 2 * k], r.inm[0, 2 * k + 1]), paired(r.inm[1, 2 * k], r.inm[1, 2 * k + 1])
        br, bi = cmul(r.fac[0, pl.ds(k, 1), :], r.fac[1, pl.ds(k, 1), :], br, bi)
        p = stacked(*outer(0, k, br, bi))
        r.pb[k] = p
        s = jnp.dot(inputs_of(k), p, preferred_element_type=F32)
        at = pl.ds(k, CH, stride=PAIRS)
        r.sr[at, :] = s[:, :128]
        r.si[at, :] = s[:, 128:]
        return 0

    lax.fori_loop(0, PAIRS, states_in, 0, unroll=2)

    a2r, a2i = cmul(ar, ai, ar, ai)
    a4r, a4i = cmul(a2r, a2i, a2r, a2i)
    a8r, a8i = cmul(a4r, a4i, a4r, a4i)

    def advance(c, carry, keep):
        vr, vi, e_all = carry
        at = pl.ds(pl.multiple_of(c * PAIRS, PAIRS), PAIRS)
        e = r.e7[at, :]
        tr, ti = (vr + r.sr[at, :]) * e, (vi + r.si[at, :]) * e
        if keep:
            r.sr[at, :], r.si[at, :] = vr, vi
        vr, vi = cmul(a8r, a8i, tr, ti)
        return vr, vi, e_all * e

    vr, vi, e_all = lax.fori_loop(0, CH, functools.partial(advance, keep=False), (zero, zero, one), unroll=8)

    causal = (iota((256, 256), 0) // 16) % Q <= (iota((256, 256), 1) // 16) % Q

    def inside(k, _):
        cr, ci = paired(r.outm[0, 2 * k], r.outm[0, 2 * k + 1]), paired(r.outm[1, 2 * k], r.outm[1, 2 * k + 1])
        qr, qi = outer(2, k, cr, ci)
        q = stacked(qr, -qi)
        r.qb[k] = q
        m = lax.dot_general(r.pb[k], q, NT, preferred_element_type=F32)
        m = jnp.where(causal, m, 0.0).astype(BF16)
        out = jnp.dot(inputs_of(k), m, preferred_element_type=F32)
        r.y[2 * k] = out[:, :128]
        r.y[2 * k + 1] = out[:, 128:]
        return 0

    def inside_part(n):
        cuts = (0, 12, 16)
        lax.fori_loop(cuts[n], cuts[n + 1], inside, 0, unroll=2)
        if n == 0:
            r.ex[...] = spread_out(jnp.exp(d))

    vr, vi = comm(ar, ai, vr, vi, e_all, inside_part)
    lax.fori_loop(0, CH, functools.partial(advance, keep=True), (vr, vi, one), unroll=8)

    def outputs(k, _):
        at = pl.ds(k, CH, stride=PAIRS)
        v = jnp.concatenate([r.sr[at, :], r.si[at, :]], axis=1).astype(BF16)
        out = lax.dot_general(v, r.qb[k], NT, preferred_element_type=F32)
        r.y[2 * k] += out[:, :128]
        r.y[2 * k + 1] += out[:, 128:]
        return 0

    lax.fori_loop(0, PAIRS, outputs, 0, unroll=2)


def finish_rows(r, q, slot):
    rows = pl.ds(pl.multiple_of(q * 128, 128), 128)

    def turn(j, _):
        parts = block_swap([r.y[j * 8 + n, pl.ds(pl.multiple_of(q * 16, 16), 16), :] for n in range(8)])
        for n in range(8):
            r.v[j, pl.ds(q * 128 + n, 16, stride=8), :] = parts[n]
        return 0

    def close(j, _):
        lanes = pl.ds(pl.multiple_of(j * 128, 128), 128)
        mixed = r.v[j, rows, :] * r.ex[rows, lanes] + r.skip[:, lanes] * r.u[rows, lanes].astype(F32)
        r.act[rows, lanes] = jax.nn.gelu(mixed).astype(BF16)
        return 0

    lax.fori_loop(0, 4, turn, 0, unroll=2)
    lax.fori_loop(0, 4, close, 0, unroll=2)


def fold(acc, vr, vi, e, wr, wi, use):
    er, ei = cmul(wr * e, wi * e, acc[0], acc[1])
    return jnp.where(use, er + vr, acc[0]), jnp.where(use, ei + vi, acc[1]), jnp.where(use, acc[2] * e, acc[2])


def squared(w, times):
    for _ in range(times):
        w = cmul(*w, *w)
    return w


class Refs:
    def __init__(self, **named):
        self.__dict__.update(named)


MIXER_SCRATCH = dict(
    steps=pltpu.VMEM((32, 64), F32), fac=pltpu.VMEM((2, PAIRS, 128), F32), pw=pltpu.VMEM((4, PAIRS * Q, 128), F32), ex=pltpu.VMEM((512, 512), F32), v=pltpu.VMEM((4, 512, 128), F32),
    e7=pltpu.VMEM((CH * PAIRS, 128), F32), z=pltpu.VMEM((32, CH, 128), F32), y=pltpu.VMEM((32, CH, 128), F32),
    pb=pltpu.VMEM((PAIRS, 256, 256), BF16), qb=pltpu.VMEM((PAIRS, 256, 256), BF16),
    sr=pltpu.VMEM((CH * PAIRS, 128), F32), si=pltpu.VMEM((CH * PAIRS, 128), F32),
)


EXCHANGE_SCRATCH = dict(
    mine=pltpu.VMEM((2, 3, PAIRS, 128), F32), got_p=pltpu.VMEM((7, 3, PAIRS, 128), F32),
    got_z=pltpu.VMEM((7, 3, PAIRS, 128), F32), ssem=pltpu.SemaphoreType.DMA((14,)), rsem=pltpu.SemaphoreType.DMA((14,)),
)


def in_plane(n):
    n = lax.rem(n, 8)
    return {"sp_1": n // 2, "sp_2": lax.rem(n, 2)}


def greet(peers):
    barrier = pltpu.get_barrier_semaphore()
    for peer in peers:
        pl.semaphore_signal(barrier, inc=1, device_id=peer, device_id_type=MESH)
    return lambda: pl.semaphore_wait(barrier, len(peers))


def exchange(r, after_own, after_inside, after_plane, ar, ai, vr, vi, e, part):
    at, z = lax.axis_index("sp_1") * 2 + lax.axis_index("sp_2"), lax.axis_index("sp_0")

    def copy(level, d, got, peer):
        n = level * 7 + d - 1
        return pltpu.make_async_remote_copy(
            src_ref=r.mine.at[level], dst_ref=got.at[d - 1], send_sem=r.ssem.at[n], recv_sem=r.rsem.at[n],
            device_id=peer, device_id_type=MESH,
        )

    def put(level, parts):
        for n, v in enumerate(parts):
            r.mine[level, n] = v

    def of(got, d):
        return got[d - 1, 0], got[d - 1, 1], got[d - 1, 2]

    nothing = (jnp.zeros_like(vr), jnp.zeros_like(vr), jnp.ones_like(vr))
    w1 = squared((ar, ai), 9)
    w8 = squared(w1, 3)
    own = (vr, vi, e)
    put(0, own)
    plane = [copy(0, d, r.got_p, in_plane(at + d)) for d in range(1, 8)]
    for d in (4, 3, 5, 2, 6, 1, 7):
        plane[d - 1].start()
    after_own()
    part(0)
    after_inside()
    for c in plane:
        c.wait()
    total = nothing
    for d in range(7, 0, -1):
        total = fold(total, *of(r.got_p, d), *w1, d <= at)
    total = fold(total, *own, *w1, True)
    for d in range(7, 0, -1):
        total = fold(total, *of(r.got_p, d), *w1, d > at)
    put(1, total)
    sends = [copy(1, d, r.got_z, {"sp_0": lax.rem(z + d, 8)}) for d in range(1, 8)]
    for d in range(1, 8):
        pl.when(z + d < 8)(sends[d - 1].start)
    after_plane()
    part(1)
    for d in range(1, 8):
        pl.when(z + d < 8)(sends[d - 1].wait_send)
        pl.when(z >= d)(sends[d - 1].wait_recv)
    enter = nothing
    for d in range(7, 0, -1):
        enter = fold(enter, *of(r.got_z, d), *w8, d <= z)
    for d in range(7, 0, -1):
        enter = fold(enter, *of(r.got_p, d), *w1, d <= at)
    return enter[0], enter[1]


class Ring:
    def __init__(self, axis, count, many, chunk, others, sent, rsem, swap=False, shared=None):
        self.axis, self.count, self.many, self.chunk, self.others, self.sent, self.rsem = axis, count, many, chunk, others, sent, rsem
        self.swap, self.shared = swap, shared
        self.me, self.half = lax.axis_index(axis), count // 2

    def place(self, steps):
        return lax.rem(self.me + steps + self.count, self.count)

    def moves(self, step, i):
        for way in (0, 1):
            j = i ^ way if self.swap else i
            if step < self.half or (step == self.half and j % 2 == way):
                yield way, j

    def copy(self, step, way, j, owner):
        n = ((step - 1) * 2 + way) * self.many + j
        ref = self.chunk(self.place(owner), j)
        return pltpu.make_async_remote_copy(
            src_ref=ref, dst_ref=ref, send_sem=self.sent, recv_sem=self.rsem.at[n],
            device_id={self.axis: self.place(1 - 2 * way)}, device_id_type=MESH,
        )

    def to_partner(self, ref):
        return pltpu.make_async_remote_copy(
            src_ref=ref, dst_ref=ref, send_sem=self.shared.at[0], recv_sem=self.shared.at[1],
            device_id={"sp_2": 1 - lax.axis_index("sp_2")}, device_id_type=MESH,
        )

    def start(self, i):
        for way, j in self.moves(1, i):
            self.copy(1, way, j, 0).start()

    def service(self, step, i):
        onward = list(self.moves(step + 1, i))
        for way, j in self.moves(step, i):
            self.copy(step, way, j, (2 * way - 1) * step).wait_recv()
            if (way, j) in onward:
                self.copy(step + 1, way, j, (2 * way - 1) * step).start()
            if self.shared is not None:
                self.to_partner(self.chunk(self.place((2 * way - 1) * step), j)).start()

    def shared_wait(self):
        self.to_partner(self.others).wait_recv()

    def drain(self):
        pltpu.make_async_remote_copy(
            src_ref=self.others, dst_ref=self.others, send_sem=self.sent, recv_sem=self.rsem.at[0],
            device_id={self.axis: self.place(1)}, device_id_type=MESH,
        ).wait_send()
        if self.shared is not None:
            self.to_partner(self.others).wait_send()


class RowSum:
    def __init__(self, part, far, near, own, sent, rsem, prepare, quarter):
        self.part, self.far, self.near, self.own, self.sent, self.rsem = part, far, near, own, sent, rsem
        self.y, self.prepare, self.quarter = lax.axis_index("tp"), prepare, quarter
        self.fars = [self.copy(n, part.at[0, n], far.at[n], 1 if n < 2 else 3) for n in range(4)]
        self.nears = [
            self.copy(4, part.at[1, pl.ds(2, 2)], near.at[0, pl.ds(2, 2)], 1), self.copy(5, part.at[2, pl.ds(0, 2)], near.at[1, pl.ds(0, 2)], 3)
        ]
        self.sums = [self.copy(6 + n, part.at[1 + n // 2, n], near.at[n // 2, n], 1 if n < 2 else 3) for n in range(4)]

    def copy(self, n, src, dst, d):
        return pltpu.make_async_remote_copy(
            src_ref=src, dst_ref=dst, send_sem=self.sent, recv_sem=self.rsem.at[n],
            device_id={"tp": lax.rem(self.y + d, 4)}, device_id_type=MESH,
        )

    def make(self, slot, d, *order):
        for n in order:
            self.part[slot, n] = self.quarter(lax.rem(self.y + d, 4), n, slot).astype(BF16)

    def others(self, busy):
        self.prepare(lax.rem(self.y + 2, 4), 0)
        for pair in ((0, 2), (1, 3)):
            self.make(0, 2, *pair)
            for n in pair:
                self.fars[n].start()
        busy(0)
        self.prepare(lax.rem(self.y + 1, 4), 1)
        self.make(1, 1, 2, 3)
        self.nears[0].start()
        busy(1)
        self.prepare(lax.rem(self.y + 3, 4), 2)
        self.make(2, 3, 0, 1)
        self.nears[1].start()
        self.make(2, 3, 2, 3)
        self.make(1, 1, 0, 1)
        busy(2)

    def mine(self):
        self.prepare(self.y, 3)
        for n in range(4):
            self.own[n] = self.quarter(self.y, n, 3)

    def pass_on(self):
        for n in (0, 2, 1, 3):
            self.fars[n].wait_recv()
            slot = 1 + n // 2
            self.part[slot, n] = (self.part[slot, n].astype(F32) + self.far[n].astype(F32)).astype(BF16)
            self.sums[n].start()

    def arrived(self):
        for c in self.nears + self.sums:
            c.wait_recv()

    def total(self, n, at):
        return self.own[n][at] + self.near[0, n][at].astype(F32) + self.near[1, n][at].astype(F32)

    def drain(self):
        self.copy(0, self.part, self.part, 1).wait_send()


def sems(n):
    return pltpu.SemaphoreType.DMA((n,))


IN_VMEM = dict(
    u=((512, 512), BF16), damp=((32, 512), F32), ls=((1, 32), F32), rr=((32, 64), F32), ri=((32, 64), F32), inm=((2, 32, 16, 64), F32),
    outm=((2, 32, 16, 64), F32), skip=((1, 512), F32), residual=((128, 2048), BF16), gain=((1, 2048), F32), taps=((3, 2, 1408), F32),
    w_out=((512, 2048), BF16),
)
EARLY = ("u", "damp", "ls", "rr", "ri", "inm", "outm", "skip")
WEIGHTS = ("w_act", "w_lin", "w_dn")
LAYER_SCRATCH = dict(
    act=pltpu.VMEM((512, 512), BF16), g=pltpu.VMEM((3, 8, 4, 2, 32, 1408), BF16), load=sems(4), result=pltpu.VMEM((128, 2048), BF16),
    stream=pltpu.VMEM((128, 2048), BF16), normed=pltpu.VMEM((33, 16, 2048), BF16),
    pre=pltpu.VMEM((2, 528, 1408), BF16), hidden=pltpu.VMEM((3, 128, 1408), BF16),
    part1=pltpu.VMEM((3, 4, 128, 512), BF16), far1=pltpu.VMEM((4, 128, 512), BF16), near1=pltpu.VMEM((2, 4, 128, 512), BF16),
    own1=pltpu.VMEM((4, 128, 512), F32), sum1_r=sems(10),
    part2=pltpu.VMEM((3, 4, 512, 128), BF16), far2=pltpu.VMEM((4, 512, 128), BF16), near2=pltpu.VMEM((2, 4, 512, 128), BF16),
    own2=pltpu.VMEM((4, 512, 128), F32), sum2_r=sems(10),
    sent=sems(7), ax_r=sems(8), bz_r=sems(16), az_r=sems(32), bx_r=sems(32), ny_r=sems(8), azp=sems(2), bxp=sems(2),
    half_s=sems(2), half_r=sems(2), halo_s=sems(4), halo_r=sems(1),
)
SCRATCH = {**MIXER_SCRATCH, **EXCHANGE_SCRATCH, **LAYER_SCRATCH}


def layer_kernel(*refs):
    given = dict(zip((*IN_VMEM, *WEIGHTS), refs))
    target = refs[len(given)]
    scratch = refs[len(given) + 1 :]
    r = Refs(**dict(zip(IN_VMEM, scratch)), **dict(zip(SCRATCH, scratch[len(IN_VMEM) :])))
    core, x, z, y = (lax.axis_index(a) for a in ("sp_2", "sp_1", "sp_0", "tp"))
    at = z * 8 + x * 2 + core

    def position(n, tp):
        n = lax.rem(n, 64)
        return {"sp_0": n // 8, "sp_1": lax.rem(n, 8) // 2, "sp_2": lax.rem(n, 2), "tp": tp}

    loads = [pltpu.make_async_copy(given[name], getattr(r, name), r.load.at[0 if name in EARLY else 1]) for name in IN_VMEM]
    weights = [pltpu.make_async_copy(given[w], r.g.at[m, z, x, core], r.load.at[2]) for m, w in enumerate(WEIGHTS)]
    for c in loads[: len(EARLY)] + weights + loads[len(EARLY) :]:
        c.start()
    r.got_z[...] = jnp.zeros_like(r.got_z)
    r.normed[0] = jnp.zeros((16, 2048), BF16)
    peers = [in_plane(x * 2 + core + d) for d in range(1, 8)]
    peers += [{axis: lax.rem(lax.axis_index(axis) + d, count)} for axis, count in (("sp_0", 8), ("tp", 4)) for d in range(1, count)]
    peers += [position(at + n, q) for n in (1, 63) for q in range(4)]
    wait_for_all = greet(peers)
    for c in loads[: len(EARLY)]:
        c.wait()

    a_cols, b_cols = pl.ds(0, 640), pl.ds(640, 768)
    a_half, b_half = (pl.ds(0, 384), pl.ds(384, 256)), (pl.ds(640, 384), pl.ds(1024, 384))
    beside_x = [lax.rem(x + n, 4) for n in (0, 1, 3, 2)]
    beside_z = [lax.rem(z + n, 8) for n in (0, 1, 7, 2, 6, 3, 5, 4)]
    ax = Ring("sp_1", 4, 2, lambda o, j: r.g.at[:, z, o, core, :, a_half[j]], r.g.at[:, z, pl.ds(0, 3), core, :, a_cols], r.sent.at[0], r.ax_r, True)
    bz = Ring("sp_0", 8, 2, lambda o, j: r.g.at[:, o, x, core, :, b_half[j]], r.g.at[:, pl.ds(0, 7), x, core, :, b_cols], r.sent.at[1], r.bz_r, True)
    az = Ring("sp_0", 8, 4, lambda o, j: r.g.at[:, o, beside_x[j], core, :, a_cols], r.g.at[:, pl.ds(0, 7), :, core, :, a_cols], r.sent.at[2], r.az_r, False, r.azp)
    bx = Ring("sp_1", 4, 8, lambda o, j: r.g.at[:, beside_z[j], o, core, :, b_cols], r.g.at[:, :, pl.ds(0, 3), core, :, b_cols], r.sent.at[3], r.bx_r, False, r.bxp)
    ny = Ring("tp", 4, 2, lambda o, j: r.normed.at[pl.ds(1 + o * 8 + j * 4, 4)], r.normed.at[pl.ds(0, 24)], r.sent.at[4], r.ny_r, True)

    def half_copies(c):
        return [
            pltpu.make_async_remote_copy(
                src_ref=ref, dst_ref=ref, send_sem=r.half_s.at[n], recv_sem=r.half_r.at[n], device_id={"sp_2": 1 - core}, device_id_type=MESH
            )
            for n, ref in enumerate((r.g.at[:, z, :, c, :, a_cols], r.g.at[:, :, x, c, :, b_cols]))
        ]

    def serve(*steps):
        for ring, step, i in steps:
            ring.service(step, i)

    def greeted():
        for c in weights:
            c.wait()
        wait_for_all()
        for i in (0, 1):
            ax.start(i)
            bz.start(i)
        az.start(0)

    def after_inside():
        serve((ax, 1, 0), (ax, 1, 1), (bz, 1, 0), (bz, 1, 1))

    def after_plane():
        for j in (1, 2):
            az.start(j)
            bx.start(j)

    mixer_phase(r, greeted, functools.partial(exchange, r, lambda: bx.start(0), after_inside, after_plane))

    for c in loads[len(EARLY) :]:
        c.wait()

    def project(b, n, slot):
        rows = pl.ds(pl.multiple_of(b * 128, 128), 128)
        return jnp.dot(r.act[rows, :], r.w_out[:, pl.ds(n * 512, 512)], preferred_element_type=F32)

    def while_projecting(slot):
        if slot == 0:
            serve((bz, 2, 0), (bz, 2, 1))
            bx.start(3)
            bx.start(4)
            serve((ax, 2, 0))
            az.start(3)
            serve((az, 1, 0))
        elif slot == 1:
            serve((bx, 1, 0))

    first = RowSum(r.part1, r.far1, r.near1, r.own1, r.sent.at[5], r.sum1_r, functools.partial(finish_rows, r), project)
    first.others(while_projecting)
    first.mine()
    serve((az, 1, 1), (bx, 1, 1))
    first.pass_on()
    serve((az, 1, 2), (bx, 1, 2), (bz, 3, 0), (bz, 3, 1))
    bx.start(5)
    bx.start(6)
    serve((az, 1, 3), (bx, 2, 0), (az, 2, 0), (bx, 1, 3), (bx, 2, 1), (az, 2, 1), (bx, 1, 4))
    first.arrived()

    def add_up(n, squares):
        cols = pl.ds(pl.multiple_of(n * 512, 512), 512)
        total = r.residual[:, cols].astype(F32) + first.total(n, ...)
        total = total.astype(BF16)
        r.stream[:, cols] = total
        total = total.astype(F32)
        return squares + total * total

    squares = lax.fori_loop(0, 4, add_up, jnp.zeros((128, 512), F32))
    scale = lax.rsqrt(jnp.sum(squares, axis=1, keepdims=True) / 2048 + 1e-06)

    def normalize(n, _):
        cols = pl.ds(pl.multiple_of(n * 256, 256), 256)
        v = (r.stream[:, cols].astype(F32) * scale * r.gain[:, cols]).astype(BF16)
        r.normed[pl.ds(1 + 8 * y, 8), :, cols] = v.reshape(8, 16, 256)
        return 0

    lax.fori_loop(0, 8, normalize, 0)
    halos = [
        pltpu.make_async_remote_copy(
            src_ref=r.normed.at[32, pl.ds(8, 8)], dst_ref=r.normed.at[0, pl.ds(8, 8)], send_sem=r.halo_s.at[q], recv_sem=r.halo_r.at[0],
            device_id=position(at + 1, q), device_id_type=MESH,
        )
        for q in range(4)
    ]
    ends = jnp.logical_and(y == 3, at < 63)

    @pl.when(ends)
    def _():
        for c in halos:
            c.start()

    ny.start(0)
    ny.start(1)
    serve((bz, 4, 0))
    bx.start(7)
    for c in half_copies(core):
        c.start()
    serve((az, 2, 2), (bx, 2, 2), (az, 2, 3), (bx, 2, 3), (bx, 1, 5), (bx, 1, 6), (az, 3, 0), (bx, 2, 4), (bx, 1, 7), (az, 3, 1), (ny, 1, 0))
    serve((bx, 2, 5), (az, 3, 2), (bx, 2, 6), (bx, 2, 7), (az, 3, 3), (az, 4, 0), (az, 4, 1), (az, 4, 2), (az, 4, 3))
    for c in half_copies(1 - core):
        c.wait_recv()
    pl.when(at > 0)(halos[0].wait_recv)
    bx.shared_wait()
    serve((ny, 1, 1), (ny, 2, 0))

    def up(w):
        return jnp.dot(r.normed[...].reshape(528, 2048), w, preferred_element_type=F32).astype(BF16)

    def up_tile(first, n, _):
        m, cols = n % 2, pl.ds(pl.multiple_of(first + (n // 2) * 256, 128), 256)
        r.pre[m, :, cols] = up(r.g[m, :, :, :, :, cols].reshape(2048, 256))
        return 0

    lax.fori_loop(0, 6, functools.partial(up_tile, 640), 0, unroll=2)
    az.shared_wait()
    lax.fori_loop(0, 4, functools.partial(up_tile, 0), 0, unroll=2)
    tail = pl.ds(512, 128)

    def up_tail(m, _):
        r.pre[m, :, tail] = up(r.g[m, :, :, :, :, tail].reshape(2048, 128))
        return 0

    lax.fori_loop(0, 2, up_tail, 0, unroll=2)

    def convolved(b, m, cols):
        v = r.pre[m, pl.ds(pl.multiple_of(b * 128, 128), 144), cols].astype(F32)
        return sum(r.taps[k, pl.ds(m, 1), cols] * v[14 + k : 142 + k] for k in range(3))

    def hide(b, slot):
        def tile(cols):
            a, l = convolved(b, 0, cols), convolved(b, 1, cols)
            r.hidden[slot % 3, :, cols] = (a / (1.0 + jnp.exp(-a)) * l).astype(BF16)

        def pair(n, _):
            for half in (0, 1):
                tile(pl.ds(pl.multiple_of(n * 256 + half * 128, 128), 128))
            return 0

        lax.fori_loop(0, 5, pair, 0)
        tile(pl.ds(1280, 128))

    def down(b, n, slot):
        w = r.g[2, pl.ds(2 * n, 2)].reshape(512, 1408)
        return lax.dot_general(w, r.hidden[slot % 3], NT, preferred_element_type=F32)

    second = RowSum(r.part2, r.far2, r.near2, r.own2, r.sent.at[6], r.sum2_r, hide, down)
    second.others(lambda slot: None)
    second.pass_on()
    second.mine()
    for c in second.nears:
        c.wait_recv()
    results = []
    for n in (0, 2, 1, 3):
        second.sums[n].wait_recv()
        cols = pl.ds(n * 512, 512)
        total = jnp.transpose(second.total(n, ...))
        r.result[:, cols] = (r.stream[:, cols].astype(F32) + total).astype(BF16)
        results.append(pltpu.make_async_copy(r.result.at[:, cols], target.at[:, cols], r.load.at[3]))
        results[-1].start()
    for ring in (ax, bz, az, bx, ny):
        ring.drain()
    for c in half_copies(core):
        c.wait_send()
    first.drain()
    second.drain()

    @pl.when(ends)
    def _():
        for c in halos:
            c.wait_send()

    for c in results:
        c.wait()


def per_device(
    mixer_input, residual, log_step, rate_real, rate_imag, damping, in_map, out_map, skip, w_out, norm_gain, w_act, w_lin, conv_taps, w_down
):
    given = (
        mixer_input, damping.T, log_step[None], rate_real, rate_imag, in_map.transpose(0, 1, 3, 2), out_map, skip[None], residual,
        norm_gain[None], conv_taps.transpose(1, 0, 2), w_out, w_act, w_lin, w_down.T,
    )
    return pl.pallas_call(
        layer_kernel,
        out_shape=jax.ShapeDtypeStruct(residual.shape, BF16),
        in_specs=[pl.BlockSpec(memory_space=pl.ANY)] * len(given),
        out_specs=pl.BlockSpec(memory_space=pl.ANY),
        scratch_shapes=[pltpu.VMEM(*v) for v in IN_VMEM.values()] + list(SCRATCH.values()),
        compiler_params=pltpu.CompilerParams(collective_id=0, has_side_effects=True, vmem_limit_bytes=60 * 2**20),
        name="layer",
    )(*given)


def solution(mesh):
    split = Mesh(mesh.devices.reshape(8, 4, 2, mesh.shape["tp"]), ("sp_0", "sp_1", "sp_2", "tp"))
    in_specs = (
        P(SP, "tp"),
        P(SP_TP, None),
        P("tp"),
        P("tp", None),
        P("tp", None),
        P(SP, "tp"),
        P(None, "tp", None, None),
        P(None, "tp", None, None),
        P("tp"),
        P("tp", None),
        P(),
        P(SP, "tp"),
        P(SP, "tp"),
        P(None, None, "tp"),
        P("tp", SP),
    )
    out_specs = P(SP_TP, None)
    return jax.shard_map(
        per_device, mesh=split, in_specs=in_specs, out_specs=out_specs, check_vma=False
    )
```
